512 devices in a mesh: ep: 32 (over z, core), tp: 16 (over y, x).
Axes of the slice: x: 4, y: 4, z: 16, core: 2. Of those that a mesh axis runs over, the one named last changes fastest.
Arguments:
- query_in: bfloat16 [1024, 32768], P('tp', 'ep'), may hold values from -6 to 6
- key_in: bfloat16 [1024, 32768], P('tp', 'ep'), may hold values from -10 to 10
- value_in: bfloat16 [1024, 32768], P('tp', 'ep'), may hold values from -6 to 6
- erase_pre: bfloat16 [1024, 32768], P('tp', 'ep'), may hold values from -8 to 5
- decay_pre: bfloat16 [1024, 32768], P('tp', 'ep'), may hold values from -30 to 4.5
- mix_gain: float32 [1024], P('tp'), may hold values from 0.1 to 1.9
- expert_in: bfloat16 [8192, 2048], P('ep'), may hold values from -6 to 6
- expert_gain: float32 [2048], replicated, may hold values from 0.1 to 1.9
- routes: int32 [8192, 2], P('ep'), may hold values from 0 to 31, all different within a row; in each aligned block of 256 rows (0 to 255, 256 to 511, ...) at most 24 rows name the same one
- route_weight: float32 [8192, 2], P('ep'), may hold values from 0.1 to 1
- gate_weight: bfloat16 [32, 2048, 3584], P('ep', None, 'tp'), may hold values from -0.125 to 0.125
- up_weight: bfloat16 [32, 2048, 3584], P('ep', None, 'tp'), may hold values from -0.125 to 0.125
- down_weight: bfloat16 [32, 3584, 2048], P('ep', 'tp'), may hold values from -0.09375 to 0.09375
Outputs:
- mixer_out: bfloat16 [1024, 32768], P('tp', 'ep')
- expert_out: bfloat16 [8192, 2048], P('ep', 'tp')
The draws below stay inside these ranges and needn't reach their ends.
Inputs may be any that keep to these rules, and one draw needn't show every extreme that they name: `routes`: A row's 2 experts differ. Within the 256 rows of one index of ep, every expert is named at most 24 times; in some of these aligned blocks one expert is named exactly 24 times.
All inputs are finite; a program needn't handle non-finite values.
Results may differ from the reference program's by a relative error of at most 0.015.
Values may be sent and summed in bfloat16 or wider, within the bound.
No kernel may reach another device: no remote copies, remote signals or barrier semaphores. Data moves between devices by JAX's collectives and lax.ppermute only.
A program may use at most 64 MiB of HBM per device.

```python
import math
import jax
import jax.numpy as jnp
import numpy as np
from jax import lax

D = 2048
HEADS = 16
HEAD_DIM = 64
WIDTH = 1024
FFX = 3584
TOPK = 2
BLOCK_TOKENS = 64
TOK_EP = 256
SEQ_DEV = 1024
EXPERTS = 32
CAP = 24
TOKENS = 8192
SEQUENCE_LENGTH = 32768
N_EP = 32
N_TP = 16


spike_count = 3


spike_total = 2


aligned_scale = 2.0


def head_classes(key):
    head_count = WIDTH // HEAD_DIM
    fast_count = head_count // 2
    order = jax.random.permutation(jax.random.fold_in(key, 101), head_count)
    return jnp.repeat(order < fast_count, HEAD_DIM)


def strong_cells(key):
    quick_decay_channels = head_classes(key)
    total_blocks = SEQUENCE_LENGTH // BLOCK_TOKENS
    selected_experts = jax.random.randint(jax.random.fold_in(key, 202), (spike_total,), 0, total_blocks)
    spike_token_rows = jnp.any((jnp.arange(SEQUENCE_LENGTH) // BLOCK_TOKENS)[:, None] == selected_experts[None, :], axis=1)
    return jnp.logical_or(quick_decay_channels[None, :], spike_token_rows[:, None])


def draw_key_in(key, part):
    random_keys = jax.random.split(jax.random.fold_in(key, 303), 3)
    strong = strong_cells(key)
    own_part = jnp.clip(jax.random.normal(random_keys[0], (SEQUENCE_LENGTH, WIDTH), jnp.float32), -4.0, 4.0)
    direction = jnp.clip(jax.random.normal(random_keys[1], (WIDTH,), jnp.float32), -3.0, 3.0)
    signs = (jax.random.randint(random_keys[2], (SEQUENCE_LENGTH,), 0, 2) * 2 - 1).astype(jnp.float32)
    shared = aligned_scale * signs[:, None] * direction[None, :]
    keys_drawn = jnp.where(strong, own_part + shared, own_part)
    return jnp.clip(keys_drawn, -10.0, 10.0).T.astype(jnp.bfloat16)


def draw_erase_pre(key, part):
    random_keys = jax.random.split(jax.random.fold_in(key, 404), 2)
    strong = strong_cells(key)
    high_value = jnp.clip(2.5 + 1.2 * jax.random.normal(random_keys[0], (SEQUENCE_LENGTH, WIDTH), jnp.float32), 0.5, 5.0)
    low_value = jnp.clip(-7.0 + 0.5 * jax.random.normal(random_keys[1], (SEQUENCE_LENGTH, WIDTH), jnp.float32), -8.0, -6.0)
    return jnp.where(strong, high_value, low_value).T.astype(jnp.bfloat16)


def draw_decay_pre(key, part):
    random_keys = jax.random.split(key, 7)
    slow_mask = jnp.logical_not(head_classes(key))
    slow_rate = jnp.log(1.0 / SEQUENCE_LENGTH) + jax.random.uniform(random_keys[1], (WIDTH,), jnp.float32, -1.0, 1.0)
    fast_rate = jax.random.uniform(random_keys[2], (WIDTH,), jnp.float32, jnp.log(1.0 / 100.0), jnp.log(1.0 / 30.0))
    base_rate = jnp.where(slow_mask, slow_rate, fast_rate)
    device_shift = jnp.repeat(jax.random.uniform(random_keys[3], (SEQUENCE_LENGTH // SEQ_DEV, 1), jnp.float32, -0.7, 0.7), SEQ_DEV, axis=0)
    jitter = jnp.clip(jax.random.normal(random_keys[4], (SEQUENCE_LENGTH, WIDTH), jnp.float32), -3.0, 3.0) * 0.6
    logarithm_rate = jnp.minimum(base_rate[None, :] + device_shift + jitter, -1.0)
    locations = jax.random.randint(random_keys[5], (spike_count,), 0, SEQUENCE_LENGTH)
    spike_rows = jnp.any(jnp.arange(SEQUENCE_LENGTH)[:, None] == locations[None, :], axis=1)
    dropped_share = jax.random.uniform(random_keys[6], (SEQUENCE_LENGTH, WIDTH), jnp.float32, 0.2, 0.45)
    spike_rate = jnp.log(-jnp.log(1.0 - dropped_share))
    logarithm_rate = jnp.where(spike_rows[:, None], spike_rate, logarithm_rate)
    return (-jnp.log(jnp.expm1(-logarithm_rate - 0.5))).T.astype(jnp.bfloat16)


def block_levels(key, extent, shards, low, top_value):
    level = 1.0
    for axis_at, parts in shards:
        heights = jax.random.uniform(jax.random.fold_in(jax.random.fold_in(key, 6), axis_at), (parts,), jnp.float32, low / len(shards), top_value / len(shards))
        level = level * jnp.repeat(jnp.exp(heights), extent[axis_at] // parts).reshape((-1,) + (1,) * (len(extent) - 1 - axis_at))
    return level


def shared_out(rng, own, number, rows, amount, top, most, lean):
    order = jax.random.permutation(rng, amount)
    crowded, usual = load_shares(amount, rows * top, most, lean, True), load_shares(amount, rows * top, most, lean, False)
    places = jnp.arange(amount)

    def named(sizes, rotation):
        used = int((sizes > 0).sum())
        fixed = max(1, used // 4)
        passed = fixed + (places - fixed + rotation * (used - fixed)) % max(1, amount - fixed)
        return jnp.zeros((amount,), jnp.int32).at[order[jnp.where(places < fixed, places, passed)]].set(jnp.asarray(sizes, jnp.int32))

    sizes = jnp.where(number % 4 == 0, named(crowded, number // 4), named(usual, number - number // 4 - 1))
    mixed = jax.random.permutation(jax.random.fold_in(own, 3), amount)
    giver, receiver = mixed[0:amount // 2 * 2:2], mixed[1:amount // 2 * 2:2]
    slack = jnp.minimum(sizes[giver] - 1, most - sizes[receiver]) // 2
    slack = jnp.where((giver == order[0]) | (receiver == order[0]) | (sizes[receiver] == 0), 0, jnp.maximum(slack, 0))
    passed = jax.random.randint(jax.random.fold_in(own, 4), (amount // 2,), 0, 1 << 20) % (slack + 1)
    sizes = sizes.at[giver].add(-passed).at[receiver].add(passed)
    members = jnp.searchsorted(jnp.cumsum(sizes), jnp.arange(rows * top), side="right").astype(jnp.int32)
    listing = members.reshape(top, rows).T
    listing = listing[jax.random.permutation(jax.random.fold_in(own, 1), rows)]
    rotation = jax.random.randint(jax.random.fold_in(own, 2), (rows, 1), 0, top)
    return jnp.take_along_axis(listing, (jnp.arange(top)[None, :] + rotation) % top, axis=1)


def load_shares(number_of, total, limit, slope, full):
    portions = [(1 << 20) // math.isqrt(rank ** slope) + 1 for rank in range(1, number_of + 1)]
    largest = limit if full else min(limit, max(-(-total // number_of), total * portions[0] // sum(portions)))
    least = 1 if total - largest >= number_of - 1 else 0
    given, spare = [largest] + [least] * (number_of - 1), total - largest - least * (number_of - 1)
    while spare > 0:
        free = [i for i in range(1, number_of) if given[i] < largest] or [i for i in range(1, number_of) if given[i] < limit]
        mass, budget = sum([portions[i] for i in free]), spare
        for i in free:
            more = min(limit - given[i], max(1, budget * portions[i] // mass), spare)
            given[i] = given[i] + more
            spare = spare - more
    return np.array(given)


def gaussian(stream_key, dims, width, bound, cuts=(), kind=jnp.bfloat16):
    values = width * jax.random.normal(stream_key, dims, jnp.float32)
    if cuts:
        values = values * block_levels(stream_key, dims, cuts, -0.22, 0.18)
    return jnp.clip(values, -bound, bound).astype(kind)


def setup_inputs(seed: int = 0) -> dict:
    streams_of = jax.random.split(jax.random.key(seed), 14)
    query_in = gaussian(streams_of[0], (WIDTH, SEQUENCE_LENGTH), 1.0, 6.0, ((0, 16), (1, 32)))
    key_in = draw_key_in(jax.random.fold_in(streams_of[13], 71), 0)
    value_in = gaussian(streams_of[2], (WIDTH, SEQUENCE_LENGTH), 1.0, 6.0, ((0, 16), (1, 32)))
    erase_pre = draw_erase_pre(jax.random.fold_in(streams_of[13], 71), 0)
    decay_pre = draw_decay_pre(jax.random.fold_in(streams_of[13], 71), 0)
    mix_gain = jnp.clip(1.0 + 0.18 * jax.random.normal(streams_of[5], (WIDTH,), jnp.float32), 0.1, 1.9)
    expert_in = gaussian(streams_of[6], (TOKENS, D), 1.0, 6.0, ((0, 32),))
    expert_gain = jnp.clip(1.0 + 0.18 * jax.random.normal(streams_of[7], (D,), jnp.float32), 0.1, 1.9)
    routes_keys = jax.random.split(jax.random.fold_in(streams_of[8], 1), TOKENS // TOK_EP)
    routes_turns = jax.random.permutation(jax.random.fold_in(streams_of[8], 3), TOKENS // TOK_EP)
    routes = jax.vmap(lambda own, number: shared_out(jax.random.fold_in(streams_of[8], 2), own, number, TOK_EP, EXPERTS, TOPK, CAP, 2))(routes_keys, routes_turns).reshape((TOKENS, TOPK))
    route_weight = jnp.clip(0.1 + 0.9 * jax.random.uniform(streams_of[9], (TOKENS, TOPK), jnp.float32) ** block_levels(streams_of[9], (TOKENS, TOPK), ((0, 32),), -0.2, 0.2), 0.1, 1.0)
    gate_weight = gaussian(streams_of[10], (EXPERTS, D, FFX), D ** -0.5, 0.125, ((0, 32), (2, 16)))
    up_weight = gaussian(streams_of[11], (EXPERTS, D, FFX), D ** -0.5, 0.125, ((0, 32), (2, 16)))
    down_weight = gaussian(streams_of[12], (EXPERTS, FFX, D), FFX ** -0.5, 0.09375, ((0, 32), (1, 16)))
    return {"query_in": query_in, "key_in": key_in, "value_in": value_in, "erase_pre": erase_pre, "decay_pre": decay_pre, "mix_gain": mix_gain, "expert_in": expert_in, "expert_gain": expert_gain, "routes": routes, "route_weight": route_weight, "gate_weight": gate_weight, "up_weight": up_weight, "down_weight": down_weight}


highest = lax.Precision.HIGHEST

def token_terms(key_in, erase_pre, decay_pre):
    key_f = key_in.astype(jnp.float32)
    unit_key = key_f * lax.rsqrt(lax.optimization_barrier(jnp.sum(key_f * key_f, axis=-1, keepdims=True)) + 1e-05)
    eraser = unit_key * jax.nn.sigmoid(erase_pre.astype(jnp.float32))
    log_keep = -jnp.exp(-jax.nn.softplus(-decay_pre.astype(jnp.float32)) - 0.5)
    return (key_f, unit_key, eraser, log_keep)

def advance(carried, inputs):
    query_f, key_f, value_f, unit_key, eraser, keep = inputs
    seen = jnp.einsum('hvk,hk->hv', carried, unit_key, precision=highest)
    carried = carried * keep[:, None, :] - seen[:, :, None] * eraser[:, None, :] + value_f[:, :, None] * key_f[:, None, :]
    return (carried, jnp.einsum('hvk,hk->hv', carried, query_f, precision=highest))

def mixer(query_in, key_in, value_in, erase_pre, decay_pre, mix_gain):
    layout = (SEQUENCE_LENGTH, HEADS, HEAD_DIM)
    query_f = query_in.astype(jnp.float32).reshape(layout)
    value_f = value_in.astype(jnp.float32).reshape(layout)
    key_f, unit_key, eraser, log_keep = token_terms(key_in.reshape(layout), erase_pre.reshape(layout), decay_pre.reshape(layout))
    inputs = (query_f, key_f, value_f, unit_key, eraser, jnp.exp(log_keep))
    initial = jnp.zeros((HEADS, HEAD_DIM, HEAD_DIM), jnp.float32)
    _, ahead = lax.scan(advance, initial, inputs)
    _, behind = lax.scan(advance, initial, inputs, reverse=True)
    summed = ahead + behind
    center = lax.optimization_barrier(jnp.mean(summed, axis=-1, keepdims=True))
    spread = lax.optimization_barrier(jnp.mean(jnp.square(summed - center), axis=-1, keepdims=True))
    scaled = (summed - center) * lax.rsqrt(spread + HEAD_DIM * 1e-05) * mix_gain.reshape(HEADS, HEAD_DIM)
    return scaled.astype(jnp.bfloat16).reshape(SEQUENCE_LENGTH, HEADS * HEAD_DIM)

def slot_targets(routes):
    onehot = (routes[:, :, None] == jnp.arange(EXPERTS, dtype=jnp.int32)[None, None, :]).astype(jnp.int32)
    flat = onehot.reshape(-1, EXPERTS)
    before = jnp.cumsum(flat, axis=0) - flat
    slot_index = lax.optimization_barrier(jnp.sum(before * flat, axis=-1)).reshape(routes.shape)
    return routes * CAP + slot_index

def dispatch_matrix(targets, slot_total):
    matches = targets[None, :, :] == jnp.arange(slot_total, dtype=jnp.int32)[:, None, None]
    return lax.optimization_barrier(jnp.sum(matches.astype(jnp.float32), axis=-1)).astype(jnp.bfloat16)

def experts_part(expert_in, expert_gain, routes, route_weight, gate_weight, up_weight, down_weight):
    input_f = expert_in.astype(jnp.float32)
    normed = (input_f * lax.rsqrt(lax.optimization_barrier(jnp.mean(input_f * input_f, axis=-1, keepdims=True)) + 1e-06) * expert_gain).astype(jnp.bfloat16)
    targets = jax.vmap(slot_targets)(routes.reshape(N_EP, TOK_EP, TOPK))

    def fill(pack):
        selected_experts, rows = pack
        return jnp.dot(dispatch_matrix(selected_experts, EXPERTS * CAP), rows, preferred_element_type=jnp.float32).astype(jnp.bfloat16)
    buffers = lax.map(fill, (targets, normed.reshape(N_EP, TOK_EP, D)))
    buffers = buffers.reshape(N_EP, EXPERTS, CAP, D).transpose(1, 0, 2, 3).reshape(EXPERTS, N_EP * CAP, D)

    def expert(pack):
        rows, gate_mat, up_mat, down_mat = pack
        gate_sum = jnp.dot(rows, gate_mat, preferred_element_type=jnp.float32)
        up_sum = jnp.dot(rows, up_mat, preferred_element_type=jnp.float32)
        hidden = (jax.nn.silu(gate_sum) * up_sum).astype(jnp.bfloat16)
        groups = hidden.reshape(-1, N_TP, FFX // N_TP).astype(jnp.float32)
        downs = down_mat.reshape(N_TP, FFX // N_TP, D).astype(jnp.float32)
        partial_value = jnp.einsum('rjf,jfd->jrd', groups, downs).astype(jnp.bfloat16)
        partial_value = lax.optimization_barrier(partial_value)
        return lax.optimization_barrier(jnp.sum(partial_value.astype(jnp.float32), axis=0)).astype(jnp.bfloat16)
    results = lax.map(expert, (buffers, gate_weight, up_weight, down_weight)).reshape(EXPERTS, N_EP, CAP, D)
    source = (jnp.arange(TOKENS, dtype=jnp.int32) // TOK_EP)[:, None]
    slot_index = targets.reshape(TOKENS, TOPK) - routes * CAP
    picked = results[routes, source, slot_index].astype(jnp.float32)
    return lax.optimization_barrier(jnp.sum(picked * route_weight[:, :, None], axis=1)).astype(jnp.bfloat16)

def reference(query_in, key_in, value_in, erase_pre, decay_pre, mix_gain, expert_in, expert_gain, routes, route_weight, gate_weight, up_weight, down_weight):
    mixer_out = mixer(query_in.T, key_in.T, value_in.T, erase_pre.T, decay_pre.T, mix_gain).T
    expert_out = experts_part(expert_in, expert_gain, routes, route_weight, gate_weight, up_weight, down_weight)
    return (mixer_out, expert_out)
```

```python
import jax
import jax.numpy as jnp
from jax import lax
from jax.experimental import pallas as pl
from jax.experimental.pallas import tpu as pltpu
from jax.sharding import PartitionSpec as P

HEAD_DIM = 64
LANES = 128
SPAN = 128
UNROLL = 2
DECAY_SCALE = 0.6065306597126334


def mm(a, b):
    return jnp.dot(
        a.astype(jnp.bfloat16), b.astype(jnp.bfloat16), preferred_element_type=jnp.float32
    )


def mm_tn(a, b):
    return lax.dot_general(
        a.astype(jnp.bfloat16),
        b.astype(jnp.bfloat16),
        (((0,), (0,)), ((), ())),
        preferred_element_type=jnp.float32,
    )


def mm_nt(a, b):
    return lax.dot_general(
        a.astype(jnp.bfloat16),
        b.astype(jnp.bfloat16),
        (((1,), (1,)), ((), ())),
        preferred_element_type=jnp.float32,
    )


def local_kernel(
    q_ref, k_ref, v_ref, e_ref, d_ref, oloc_ref, qp_ref, maps_ref,
    uk_ref, er_ref, lk_ref, qh_f_ref, qh_b_ref, z_ref, b_ref, dec_ref,
):
    count = q_ref.shape[1] // SPAN
    kf = k_ref[...].astype(jnp.float32)
    uk = kf * lax.rsqrt(jnp.sum(kf * kf, axis=0, keepdims=True) + 1e-05)
    uk_ref[...] = uk
    er_ref[...] = uk * (1.0 / (1.0 + jnp.exp(-e_ref[...].astype(jnp.float32))))
    lk_ref[...] = -DECAY_SCALE / (1.0 + jnp.exp(-d_ref[...].astype(jnp.float32)))

    row = lax.broadcasted_iota(jnp.int32, (SPAN, SPAN), 0)
    col = lax.broadcasted_iota(jnp.int32, (SPAN, SPAN), 1)
    differ = row ^ col
    eye_span = jnp.where(differ == 0, 1.0, 0.0)
    running = jnp.where(row <= col, 1.0, 0.0).astype(jnp.bfloat16)
    eye = jnp.where(
        lax.broadcasted_iota(jnp.int32, (HEAD_DIM, HEAD_DIM), 0)
        == lax.broadcasted_iota(jnp.int32, (HEAD_DIM, HEAD_DIM), 1),
        1.0,
        0.0,
    )
    strict = (row < col, row > col)
    inclusive = (row <= col, row >= col)

    def body(step, carry):
        units = []
        for part in range(UNROLL):
            chunk = step * UNROLL + part
            lanes = pl.ds(pl.multiple_of(chunk * SPAN, SPAN), SPAN)
            q = q_ref[:, lanes].astype(jnp.float32)
            k = k_ref[:, lanes].astype(jnp.float32)
            v = v_ref[:, lanes]
            u, er, lk = uk_ref[:, lanes], er_ref[:, lanes], lk_ref[:, lanes]
            high = lk.astype(jnp.bfloat16)
            rest = lk - high.astype(jnp.float32)
            low = rest.astype(jnp.bfloat16)
            sums = mm(jnp.concatenate([high, low], axis=0), running)
            cum = sums[:HEAD_DIM] + sums[HEAD_DIM:]
            prior = cum - lk
            last = cum[:, SPAN - 1 :]
            to_prior, fade = jnp.exp(prior), jnp.exp(last - cum)
            up_f, up_b = jnp.exp(-cum), jnp.exp(prior - last)
            dec_ref[chunk] = jnp.sum(eye * jnp.exp(last), axis=0, keepdims=True)
            both = (
                (u * to_prior, q * jnp.exp(cum), k * up_f, er * up_f, k * fade, er * fade),
                (u * fade, q * jnp.exp(last - prior), k * up_b, er * up_b, k * to_prior, er * to_prior),
            )
            for way in (0, 1):
                units.append((chunk, lanes, way, v, both[way]))
        state = []
        for chunk, lanes, way, v, (ud, qd, ku, eu, kend, eend) in units:
            gram = mm_tn(
                jnp.concatenate([ku, eu], axis=1), jnp.concatenate([ud, qd], axis=1)
            )
            k_mix = jnp.where(strict[way], gram[:SPAN, :SPAN], 0.0).astype(jnp.bfloat16)
            k_read = jnp.where(inclusive[way], gram[:SPAN, SPAN:], 0.0).astype(jnp.bfloat16)
            e_mix = jnp.where(strict[way], gram[SPAN:, :SPAN], 0.0)
            e_read = jnp.where(inclusive[way], gram[SPAN:, SPAN:], 0.0).astype(jnp.bfloat16)
            inv = (eye_span - jnp.where(differ == 1, e_mix, 0.0)).astype(jnp.bfloat16)
            mixed = mm(v, jnp.concatenate([k_mix, k_read], axis=1))
            state.append([e_mix, inv, mixed, e_read])
        width = 2
        while width < SPAN:
            inside = (differ >= width) & (differ < 2 * width)
            halves = [mm(inv, jnp.where(inside, e_mix, 0.0)) for e_mix, inv, _, _ in state]
            for unit, half in zip(state, halves):
                unit[1] = (unit[1].astype(jnp.float32) - mm(half, unit[1])).astype(jnp.bfloat16)
            width *= 2
        for (chunk, lanes, way, v, (ud, qd, ku, eu, kend, eend)), (_, inv, mixed, e_read) in zip(
            units, state
        ):
            solved = mm(jnp.concatenate([ud, mixed[:, :SPAN]], axis=0), inv).astype(jnp.bfloat16)
            read = mm(solved, e_read)
            ends = mm_nt(solved, eend)
            qh = (qh_f_ref, qh_b_ref)[way]
            qh[:, lanes] = (qd - read[:HEAD_DIM]).astype(jnp.bfloat16)
            out = mixed[:, SPAN:] - read[HEAD_DIM:]
            if way == 0:
                oloc_ref[:, lanes] = out
            else:
                oloc_ref[:, lanes] += out
            z_ref[way, chunk] = ends[:HEAD_DIM].astype(jnp.bfloat16)
            b_ref[way, chunk] = mm_nt(v, kend) - ends[HEAD_DIM:]
        return carry

    lax.fori_loop(0, count // UNROLL, body, 0)

    start = jnp.concatenate([jnp.zeros_like(eye), eye], axis=0)
    carried = [start, start]
    for step in range(count):
        for way, qh in ((0, qh_f_ref), (1, qh_b_ref)):
            chunk = step if way == 0 else count - 1 - step
            lanes = slice(chunk * SPAN, (chunk + 1) * SPAN)
            now = carried[way]
            narrow = now.astype(jnp.bfloat16)
            read = mm(narrow, qh[:, lanes])
            oloc_ref[:, lanes] += read[:HEAD_DIM]
            qp_ref[way * HEAD_DIM : (way + 1) * HEAD_DIM, lanes] = read[HEAD_DIM:].astype(jnp.bfloat16)
            moved = now * dec_ref[chunk] - mm(narrow, z_ref[way, chunk])
            carried[way] = jnp.concatenate(
                [moved[:HEAD_DIM] + b_ref[way, chunk], moved[HEAD_DIM:]], axis=0
            )
    for way in (0, 1):
        maps_ref[way] = jnp.concatenate(
            [carried[way][:HEAD_DIM], carried[way][HEAD_DIM:] - eye], axis=1
        ).astype(jnp.bfloat16)


def local_half(query, key, value, erase, decay):
    tokens = query.shape[1]
    count = tokens // SPAN
    full = lambda kind: jax.ShapeDtypeStruct((HEAD_DIM, tokens), kind)
    whole = lambda kind: pltpu.VMEM((HEAD_DIM, tokens), kind)
    return pl.pallas_call(
        local_kernel,
        out_shape=(
            full(jnp.float32),
            jax.ShapeDtypeStruct((2 * HEAD_DIM, tokens), jnp.bfloat16),
            jax.ShapeDtypeStruct((2, HEAD_DIM, 2 * HEAD_DIM), jnp.bfloat16),
        ),
        scratch_shapes=[
            whole(jnp.float32),
            whole(jnp.float32),
            whole(jnp.float32),
            whole(jnp.bfloat16),
            whole(jnp.bfloat16),
            pltpu.VMEM((2, count, HEAD_DIM, HEAD_DIM), jnp.bfloat16),
            pltpu.VMEM((2, count, HEAD_DIM, HEAD_DIM), jnp.float32),
            pltpu.VMEM((count, 1, HEAD_DIM), jnp.float32),
        ],
        cost_estimate=pl.CostEstimate(
            flops=16 * 22 * 2 * 128**3, bytes_accessed=tokens * 64 * 18, transcendentals=tokens * 64 * 9
        ),
        name="mixer_local",
    )(query, key, value, erase, decay)


def finish_kernel(me_ref, got_ref, oloc_ref, qp_ref, gain_ref, out_ref):
    devices = got_ref.shape[0]
    me = me_ref[0]
    left = lax.broadcasted_iota(jnp.int32, (2 * HEAD_DIM, 2 * HEAD_DIM), 1) < HEAD_DIM
    entering = []
    for way in (0, 1):
        level = []
        for place in range(devices):
            source = place if way == 0 else devices - 1 - place
            wanted = source < me if way == 0 else source > me
            both = got_ref[source].astype(jnp.float32)
            stacked = jnp.concatenate([pltpu.roll(both, HEAD_DIM, 1), both], axis=0)
            level.append(jnp.where(left & wanted, stacked, 0.0))
        while len(level) > 1:
            level = [
                first + mm(first, later) + later
                for first, later in zip(level[::2], level[1::2])
            ]
        entering.append(level[0][HEAD_DIM:])
    states = entering[0] + pltpu.roll(entering[1], HEAD_DIM, 1)
    summed = oloc_ref[...] + mm(states, qp_ref[...])
    center = jnp.mean(summed, axis=0, keepdims=True)
    away = summed - center
    spread = jnp.mean(away * away, axis=0, keepdims=True)
    out_ref[...] = (
        away * lax.rsqrt(spread + HEAD_DIM * 1e-05) * gain_ref[...]
    ).astype(jnp.bfloat16)


def finish_half(me, got, oloc, qp, gain):
    return pl.pallas_call(
        finish_kernel,
        out_shape=jax.ShapeDtypeStruct(oloc.shape, jnp.bfloat16),
        in_specs=[pl.BlockSpec(memory_space=pltpu.SMEM)] + [pl.BlockSpec(memory_space=pltpu.VMEM)] * 4,
        cost_estimate=pl.CostEstimate(
            flops=62 * 2 * 128 * 64 * 64 + 4 * 64 * 64 * 1024, bytes_accessed=2**20, transcendentals=1024
        ),
        name="mixer_finish",
    )(me, got, oloc, qp, gain)


def expert_kernel(rows_ref, gate_ref, up_ref, down_ref, out_ref):
    parts = rows_ref.shape[0]
    rows = jnp.concatenate([rows_ref[j] for j in range(parts)], axis=1)
    gate = mm(rows, gate_ref[...])
    up = mm(rows, up_ref[...])
    hidden = (gate / (1.0 + jnp.exp(-gate)) * up).astype(jnp.bfloat16)
    result = mm(hidden, down_ref[...]).astype(jnp.bfloat16)
    for j in range(parts):
        out_ref[j] = result[:, j * LANES : (j + 1) * LANES]


def expert_rows(rows, gate, up, down):
    parts, total, lanes = rows.shape
    tile = 256 if total % 256 == 0 else total
    block = pl.BlockSpec((parts, tile, lanes), lambda i: (0, i, 0))
    fixed = lambda array: pl.BlockSpec(array.shape, lambda i: (0, 0))
    return pl.pallas_call(
        expert_kernel,
        grid=(total // tile,),
        in_specs=[block, fixed(gate), fixed(up), fixed(down)],
        out_specs=block,
        out_shape=jax.ShapeDtypeStruct(rows.shape, jnp.bfloat16),
        cost_estimate=pl.CostEstimate(
            flops=6 * total * gate.size,
            bytes_accessed=2 * (2 * rows.size + 3 * gate.size),
            transcendentals=total * gate.shape[1],
        ),
        name="expert_rows",
    )(rows, gate, up, down)


def slot_targets(routes, experts_n, capacity):
    onehot = (routes[:, :, None] == jnp.arange(experts_n, dtype=jnp.int32)[None, None, :]).astype(
        jnp.int32
    )
    flat = onehot.reshape(-1, experts_n)
    before = jnp.cumsum(flat, axis=0) - flat
    slot_index = jnp.sum(before * flat, axis=-1).reshape(routes.shape)
    return routes * capacity + slot_index


def dispatch_matrix(targets, slot_total):
    matches = targets[None, :, :] == jnp.arange(slot_total, dtype=jnp.int32)[:, None, None]
    return jnp.sum(matches.astype(jnp.float32), axis=-1).astype(jnp.bfloat16)


def spread(array, axis):
    return lax.all_to_all(array, axis, 0, 0, tiled=True)


def on_device(
    query_in,
    key_in,
    value_in,
    erase_pre,
    decay_pre,
    mix_gain,
    expert_in,
    expert_gain,
    routes,
    route_weight,
    gate_weight,
    up_weight,
    down_weight,
):
    experts_n, shares = lax.axis_size("ep"), lax.axis_size("tp")
    row_count, features = expert_in.shape
    capacity = 3 * routes.shape[1] * row_count // (2 * experts_n)
    slot_total = experts_n * capacity
    col_count = features // shares
    at = lax.axis_index("tp") * col_count
    input_f = expert_in.astype(jnp.float32)
    scale = lax.rsqrt(jnp.mean(input_f * input_f, axis=-1, keepdims=True) + 1e-06)
    own = lax.dynamic_slice_in_dim(expert_in, at, col_count, 1).astype(jnp.float32)
    normed = (own * scale * lax.dynamic_slice_in_dim(expert_gain, at, col_count, 0)).astype(
        jnp.bfloat16
    )
    targets = slot_targets(routes, experts_n, capacity)
    outgoing = mm(dispatch_matrix(targets, slot_total), normed).astype(jnp.bfloat16)
    arrived = spread(outgoing.reshape(experts_n, capacity, col_count), "ep").reshape(
        slot_total, col_count
    )
    shared = spread(jnp.broadcast_to(arrived[None], (shares, *arrived.shape)), "tp")

    oloc, qp, maps = local_half(query_in, key_in, value_in, erase_pre, decay_pre)
    me = lax.axis_index("ep")
    later = jnp.arange(experts_n) > me
    outgoing = jnp.where(later[:, None, None], maps[:1], maps[1:])

    shared, outgoing = lax.optimization_barrier((shared, outgoing))
    partial = expert_rows(shared, gate_weight[0], up_weight[0], down_weight[0])
    got = spread(outgoing, "ep")
    partial, got = lax.optimization_barrier((partial, got))
    pieces = spread(partial, "tp")
    summed = jnp.sum(pieces.astype(jnp.float32), axis=0).astype(jnp.bfloat16)
    returned = spread(summed.reshape(experts_n, capacity, col_count), "ep").reshape(
        slot_total, col_count
    )
    mixer_out = finish_half(
        me.reshape(1).astype(jnp.int32), got, oloc, qp, mix_gain[:, None]
    )
    matches = targets[:, :, None] == jnp.arange(slot_total, dtype=jnp.int32)[None, None, :]
    combine = jnp.sum(matches.astype(jnp.float32) * route_weight[:, :, None], axis=1)
    expert_out = jnp.dot(combine, returned.astype(jnp.float32)).astype(jnp.bfloat16)
    return (mixer_out, expert_out)


def solution(mesh):
    placed = (
        P("tp", "ep"),
        P("tp", "ep"),
        P("tp", "ep"),
        P("tp", "ep"),
        P("tp", "ep"),
        P("tp"),
        P("ep", None),
        P(),
        P("ep", None),
        P("ep", None),
        P("ep", None, "tp"),
        P("ep", None, "tp"),
        P("ep", "tp", None),
    )
    return jax.shard_map(
        on_device,
        mesh=mesh,
        in_specs=placed,
        out_specs=(P("tp", "ep"), P("ep", "tp")),
        check_vma=False,
    )
```

```python
import jax
import jax.numpy as jnp
from jax import lax
from jax.experimental import pallas as pl
from jax.experimental.pallas import tpu as pltpu
from jax.sharding import PartitionSpec as P

HEAD_DIM = 64
LANES = 128
SPAN = 128
UNROLL = 2
DECAY_SCALE = 0.6065306597126334


def mm(a, b):
    return jnp.dot(
        a.astype(jnp.bfloat16), b.astype(jnp.bfloat16), preferred_element_type=jnp.float32
    )


def mm_tn(a, b):
    return lax.dot_general(
        a.astype(jnp.bfloat16),
        b.astype(jnp.bfloat16),
        (((0,), (0,)), ((), ())),
        preferred_element_type=jnp.float32,
    )


def mm_nt(a, b):
    return lax.dot_general(
        a.astype(jnp.bfloat16),
        b.astype(jnp.bfloat16),
        (((1,), (1,)), ((), ())),
        preferred_element_type=jnp.float32,
    )


def local_kernel(
    q_ref, k_ref, v_ref, e_ref, d_ref, oloc_ref, qp_ref, maps_ref,
    uk_ref, er_ref, lk_ref, qh_f_ref, qh_b_ref, z_ref, b_ref, dec_ref,
):
    count = q_ref.shape[1] // SPAN
    kf = k_ref[...].astype(jnp.float32)
    uk = kf * lax.rsqrt(jnp.sum(kf * kf, axis=0, keepdims=True) + 1e-05)
    uk_ref[...] = uk
    er_ref[...] = uk * (1.0 / (1.0 + jnp.exp(-e_ref[...].astype(jnp.float32))))
    lk_ref[...] = -DECAY_SCALE / (1.0 + jnp.exp(-d_ref[...].astype(jnp.float32)))

    row = lax.broadcasted_iota(jnp.int32, (SPAN, SPAN), 0)
    col = lax.broadcasted_iota(jnp.int32, (SPAN, SPAN), 1)
    differ = row ^ col
    eye_span = jnp.where(differ == 0, 1.0, 0.0)
    running = jnp.where(row <= col, 1.0, 0.0).astype(jnp.bfloat16)
    eye = jnp.where(
        lax.broadcasted_iota(jnp.int32, (HEAD_DIM, HEAD_DIM), 0)
        == lax.broadcasted_iota(jnp.int32, (HEAD_DIM, HEAD_DIM), 1),
        1.0,
        0.0,
    )
    strict = (row < col, row > col)
    inclusive = (row <= col, row >= col)

    def body(step, carry):
        units = []
        for part in range(UNROLL):
            chunk = step * UNROLL + part
            lanes = pl.ds(pl.multiple_of(chunk * SPAN, SPAN), SPAN)
            q = q_ref[:, lanes].astype(jnp.float32)
            k = k_ref[:, lanes].astype(jnp.float32)
            v = v_ref[:, lanes]
            u, er, lk = uk_ref[:, lanes], er_ref[:, lanes], lk_ref[:, lanes]
            high = lk.astype(jnp.bfloat16)
            rest = lk - high.astype(jnp.float32)
            low = rest.astype(jnp.bfloat16)
            sums = mm(jnp.concatenate([high, low], axis=0), running)
            cum = sums[:HEAD_DIM] + sums[HEAD_DIM:]
            prior = cum - lk
            last = cum[:, SPAN - 1 :]
            to_prior, fade = jnp.exp(prior), jnp.exp(last - cum)
            up_f, up_b = jnp.exp(-cum), jnp.exp(prior - last)
            dec_ref[chunk] = jnp.sum(eye * jnp.exp(last), axis=0, keepdims=True)
            both = (
                (u * to_prior, q * jnp.exp(cum), k * up_f, er * up_f, k * fade, er * fade),
                (u * fade, q * jnp.exp(last - prior), k * up_b, er * up_b, k * to_prior, er * to_prior),
            )
            for way in (0, 1):
                units.append((chunk, lanes, way, v, both[way]))
        state = []
        for chunk, lanes, way, v, (ud, qd, ku, eu, kend, eend) in units:
            gram = mm_tn(
                jnp.concatenate([ku, eu], axis=1), jnp.concatenate([ud, qd], axis=1)
            )
            k_mix = jnp.where(strict[way], gram[:SPAN, :SPAN], 0.0).astype(jnp.bfloat16)
            k_read = jnp.where(inclusive[way], gram[:SPAN, SPAN:], 0.0).astype(jnp.bfloat16)
            e_mix = jnp.where(strict[way], gram[SPAN:, :SPAN], 0.0)
            e_read = jnp.where(inclusive[way], gram[SPAN:, SPAN:], 0.0).astype(jnp.bfloat16)
            inv = (eye_span - jnp.where(differ == 1, e_mix, 0.0)).astype(jnp.bfloat16)
            mixed = mm(v, jnp.concatenate([k_mix, k_read], axis=1))
            state.append([e_mix, inv, mixed, e_read])
        width = 2
        while width < SPAN:
            inside = (differ >= width) & (differ < 2 * width)
            halves = [mm(inv, jnp.where(inside, e_mix, 0.0)) for e_mix, inv, _, _ in state]
            for unit, half in zip(state, halves):
                unit[1] = (unit[1].astype(jnp.float32) - mm(half, unit[1])).astype(jnp.bfloat16)
            width *= 2
        for (chunk, lanes, way, v, (ud, qd, ku, eu, kend, eend)), (_, inv, mixed, e_read) in zip(
            units, state
        ):
            solved = mm(jnp.concatenate([ud, mixed[:, :SPAN]], axis=0), inv).astype(jnp.bfloat16)
            read = mm(solved, e_read)
            ends = mm_nt(solved, eend)
            qh = (qh_f_ref, qh_b_ref)[way]
            qh[:, lanes] = (qd - read[:HEAD_DIM]).astype(jnp.bfloat16)
            out = mixed[:, SPAN:] - read[HEAD_DIM:]
            if way == 0:
                oloc_ref[:, lanes] = out
            else:
                oloc_ref[:, lanes] += out
            z_ref[way, chunk] = ends[:HEAD_DIM].astype(jnp.bfloat16)
            b_ref[way, chunk] = mm_nt(v, kend) - ends[HEAD_DIM:]
        return carry

    lax.fori_loop(0, count // UNROLL, body, 0)

    start = jnp.concatenate([jnp.zeros_like(eye), eye], axis=0)
    carried = [start, start]
    for step in range(count):
        for way, qh in ((0, qh_f_ref), (1, qh_b_ref)):
            chunk = step if way == 0 else count - 1 - step
            lanes = slice(chunk * SPAN, (chunk + 1) * SPAN)
            now = carried[way]
            narrow = now.astype(jnp.bfloat16)
            read = mm(narrow, qh[:, lanes])
            oloc_ref[:, lanes] += read[:HEAD_DIM]
            qp_ref[way * HEAD_DIM : (way + 1) * HEAD_DIM, lanes] = read[HEAD_DIM:].astype(jnp.bfloat16)
            moved = now * dec_ref[chunk] - mm(narrow, z_ref[way, chunk])
            carried[way] = jnp.concatenate(
                [moved[:HEAD_DIM] + b_ref[way, chunk], moved[HEAD_DIM:]], axis=0
            )
    for way in (0, 1):
        maps_ref[way] = jnp.concatenate(
            [carried[way][:HEAD_DIM], carried[way][HEAD_DIM:] - eye], axis=1
        ).astype(jnp.bfloat16)


def local_half(query, key, value, erase, decay):
    tokens = query.shape[1]
    count = tokens // SPAN
    full = lambda kind: jax.ShapeDtypeStruct((HEAD_DIM, tokens), kind)
    whole = lambda kind: pltpu.VMEM((HEAD_DIM, tokens), kind)
    return pl.pallas_call(
        local_kernel,
        out_shape=(
            full(jnp.float32),
            jax.ShapeDtypeStruct((2 * HEAD_DIM, tokens), jnp.bfloat16),
            jax.ShapeDtypeStruct((2, HEAD_DIM, 2 * HEAD_DIM), jnp.bfloat16),
        ),
        scratch_shapes=[
            whole(jnp.float32),
            whole(jnp.float32),
            whole(jnp.float32),
            whole(jnp.bfloat16),
            whole(jnp.bfloat16),
            pltpu.VMEM((2, count, HEAD_DIM, HEAD_DIM), jnp.bfloat16),
            pltpu.VMEM((2, count, HEAD_DIM, HEAD_DIM), jnp.float32),
            pltpu.VMEM((count, 1, HEAD_DIM), jnp.float32),
        ],
        cost_estimate=pl.CostEstimate(
            flops=16 * 22 * 2 * 128**3, bytes_accessed=tokens * 64 * 18, transcendentals=tokens * 64 * 9
        ),
        name="mixer_local",
    )(query, key, value, erase, decay)


def stacked(wide):
    left = lax.broadcasted_iota(jnp.int32, (2 * HEAD_DIM, 2 * HEAD_DIM), 1) < HEAD_DIM
    full = wide.astype(jnp.float32)
    return jnp.where(left, jnp.concatenate([pltpu.roll(full, HEAD_DIM, 1), full], axis=0), 0.0)


def widened(tall):
    return tall[HEAD_DIM:] + pltpu.roll(tall[:HEAD_DIM], HEAD_DIM, 1)


def composed(first, later):
    return first + mm(first, later) + later


def step_kernel(arrived_f_ref, arrived_b_ref, past_ref, own_ref, next_past_ref, through_ref):
    for way, arrived in ((0, arrived_f_ref), (1, arrived_b_ref)):
        past = composed(stacked(arrived[...]), stacked(past_ref[way]))
        next_past_ref[way] = widened(past)
        through_ref[way] = widened(composed(past, stacked(own_ref[way]))).astype(jnp.bfloat16)


def scan_step(arrived, past, own):
    return pl.pallas_call(
        step_kernel,
        out_shape=(
            jax.ShapeDtypeStruct(past.shape, jnp.float32),
            jax.ShapeDtypeStruct(past.shape, jnp.bfloat16),
        ),
        cost_estimate=pl.CostEstimate(
            flops=8 * 128**3, bytes_accessed=6 * 2 * past.size, transcendentals=0
        ),
        name="scan_step",
    )(*arrived, past, own)


def finish_kernel(arrived_f_ref, arrived_b_ref, past_ref, oloc_ref, qp_ref, gain_ref, out_ref):
    entering = [
        composed(stacked(arrived[...]), stacked(past_ref[way]))[HEAD_DIM:]
        for way, arrived in ((0, arrived_f_ref), (1, arrived_b_ref))
    ]
    states = entering[0] + pltpu.roll(entering[1], HEAD_DIM, 1)
    summed = oloc_ref[...] + mm(states, qp_ref[...])
    center = jnp.mean(summed, axis=0, keepdims=True)
    away = summed - center
    spread = jnp.mean(away * away, axis=0, keepdims=True)
    out_ref[...] = (
        away * lax.rsqrt(spread + HEAD_DIM * 1e-05) * gain_ref[...]
    ).astype(jnp.bfloat16)


def finish_half(arrived, past, oloc, qp, gain):
    return pl.pallas_call(
        finish_kernel,
        out_shape=jax.ShapeDtypeStruct(oloc.shape, jnp.bfloat16),
        cost_estimate=pl.CostEstimate(
            flops=4 * 128**3 + 16 * 128**3, bytes_accessed=2**20, transcendentals=1024
        ),
        name="mixer_finish",
    )(*arrived, past, oloc, qp, gain)


def passed_on(through, distance):
    count = lax.axis_size("ep")
    ahead = [(i, i + distance) for i in range(count - distance)]
    back = [(i + distance, i) for i in range(count - distance)]
    return lax.ppermute(through[0], "ep", ahead), lax.ppermute(through[1], "ep", back)


def expert_kernel(rows_ref, gate_ref, up_ref, down_ref, out_ref):
    parts = rows_ref.shape[0]
    rows = jnp.concatenate([rows_ref[j] for j in range(parts)], axis=1)
    gate = mm(rows, gate_ref[...])
    up = mm(rows, up_ref[...])
    hidden = (gate / (1.0 + jnp.exp(-gate)) * up).astype(jnp.bfloat16)
    result = mm(hidden, down_ref[...]).astype(jnp.bfloat16)
    for j in range(parts):
        out_ref[j] = result[:, j * LANES : (j + 1) * LANES]


def expert_rows(rows, gate, up, down):
    parts, total, lanes = rows.shape
    tile = 256 if total % 256 == 0 else total
    block = pl.BlockSpec((parts, tile, lanes), lambda i: (0, i, 0))
    fixed = lambda array: pl.BlockSpec(array.shape, lambda i: (0, 0))
    return pl.pallas_call(
        expert_kernel,
        grid=(total // tile,),
        in_specs=[block, fixed(gate), fixed(up), fixed(down)],
        out_specs=block,
        out_shape=jax.ShapeDtypeStruct(rows.shape, jnp.bfloat16),
        cost_estimate=pl.CostEstimate(
            flops=6 * total * gate.size,
            bytes_accessed=2 * (2 * rows.size + 3 * gate.size),
            transcendentals=total * gate.shape[1],
        ),
        name="expert_rows",
    )(rows, gate, up, down)


def slot_targets(routes, experts_n, capacity):
    onehot = (routes[:, :, None] == jnp.arange(experts_n, dtype=jnp.int32)[None, None, :]).astype(
        jnp.int32
    )
    flat = onehot.reshape(-1, experts_n)
    before = jnp.cumsum(flat, axis=0) - flat
    slot_index = jnp.sum(before * flat, axis=-1).reshape(routes.shape)
    return routes * capacity + slot_index


def dispatch_matrix(targets, slot_total):
    matches = targets[None, :, :] == jnp.arange(slot_total, dtype=jnp.int32)[:, None, None]
    return jnp.sum(matches.astype(jnp.float32), axis=-1).astype(jnp.bfloat16)


def spread(array, axis):
    return lax.all_to_all(array, axis, 0, 0, tiled=True)


def on_device(
    query_in,
    key_in,
    value_in,
    erase_pre,
    decay_pre,
    mix_gain,
    expert_in,
    expert_gain,
    routes,
    route_weight,
    gate_weight,
    up_weight,
    down_weight,
):
    experts_n, shares = lax.axis_size("ep"), lax.axis_size("tp")
    row_count, features = expert_in.shape
    capacity = 3 * routes.shape[1] * row_count // (2 * experts_n)
    slot_total = experts_n * capacity
    col_count = features // shares
    at = lax.axis_index("tp") * col_count
    input_f = expert_in.astype(jnp.float32)
    scale = lax.rsqrt(jnp.mean(input_f * input_f, axis=-1, keepdims=True) + 1e-06)
    own = lax.dynamic_slice_in_dim(expert_in, at, col_count, 1).astype(jnp.float32)
    normed = (own * scale * lax.dynamic_slice_in_dim(expert_gain, at, col_count, 0)).astype(
        jnp.bfloat16
    )
    targets = slot_targets(routes, experts_n, capacity)
    outgoing = mm(dispatch_matrix(targets, slot_total), normed).astype(jnp.bfloat16)
    arrived = spread(outgoing.reshape(experts_n, capacity, col_count), "ep").reshape(
        slot_total, col_count
    )
    oloc, qp, own_maps = local_half(query_in, key_in, value_in, erase_pre, decay_pre)
    arrived, own_maps = lax.optimization_barrier((arrived, own_maps))
    shared = spread(jnp.broadcast_to(arrived[None], (shares, *arrived.shape)), "tp")

    past = jnp.zeros(own_maps.shape, jnp.float32)
    through, distance = own_maps, 1
    while distance < experts_n // 4:
        past, through = scan_step(passed_on(through, distance), past, own_maps)
        distance *= 2
    shared, past, through = lax.optimization_barrier((shared, past, through))
    partial = expert_rows(shared, gate_weight[0], up_weight[0], down_weight[0])
    partial, past, through = lax.optimization_barrier((partial, past, through))
    while distance < experts_n // 2:
        past, through = scan_step(passed_on(through, distance), past, own_maps)
        distance *= 2
    crossing = passed_on(through, distance)
    pieces = spread(partial, "tp")
    pieces, crossing = lax.optimization_barrier((pieces, crossing))
    summed = jnp.sum(pieces.astype(jnp.float32), axis=0).astype(jnp.bfloat16)
    returned = spread(summed.reshape(experts_n, capacity, col_count), "ep").reshape(
        slot_total, col_count
    )
    mixer_out = finish_half(crossing, past, oloc, qp, mix_gain[:, None])
    matches = targets[:, :, None] == jnp.arange(slot_total, dtype=jnp.int32)[None, None, :]
    combine = jnp.sum(matches.astype(jnp.float32) * route_weight[:, :, None], axis=1)
    expert_out = jnp.dot(combine, returned.astype(jnp.float32)).astype(jnp.bfloat16)
    return (mixer_out, expert_out)


def solution(mesh):
    placed = (
        P("tp", "ep"),
        P("tp", "ep"),
        P("tp", "ep"),
        P("tp", "ep"),
        P("tp", "ep"),
        P("tp"),
        P("ep", None),
        P(),
        P("ep", None),
        P("ep", None),
        P("ep", None, "tp"),
        P("ep", None, "tp"),
        P("ep", "tp", None),
    )
    return jax.shard_map(
        on_device,
        mesh=mesh,
        in_specs=placed,
        out_specs=(P("tp", "ep"), P("ep", "tp")),
        check_vma=False,
    )
```

```python
import jax
import jax.numpy as jnp
from jax import lax
from jax.experimental import pallas as pl
from jax.experimental.pallas import tpu as pltpu
from jax.sharding import PartitionSpec as P

HEAD_DIM = 64
LANES = 128
SPAN = 128
UNROLL = 2
DECAY_SCALE = 0.6065306597126334


def mm(a, b):
    return jnp.dot(
        a.astype(jnp.bfloat16), b.astype(jnp.bfloat16), preferred_element_type=jnp.float32
    )


def mm_tn(a, b):
    return lax.dot_general(
        a.astype(jnp.bfloat16),
        b.astype(jnp.bfloat16),
        (((0,), (0,)), ((), ())),
        preferred_element_type=jnp.float32,
    )


def mm_nt(a, b):
    return lax.dot_general(
        a.astype(jnp.bfloat16),
        b.astype(jnp.bfloat16),
        (((1,), (1,)), ((), ())),
        preferred_element_type=jnp.float32,
    )


def local_kernel(
    q_ref, k_ref, v_ref, e_ref, d_ref, oloc_ref, qp_ref, maps_ref,
    uk_ref, er_ref, lk_ref, qh_f_ref, qh_b_ref, z_ref, b_ref, dec_ref,
):
    count = q_ref.shape[1] // SPAN
    kf = k_ref[...].astype(jnp.float32)
    uk = kf * lax.rsqrt(jnp.sum(kf * kf, axis=0, keepdims=True) + 1e-05)
    uk_ref[...] = uk
    er_ref[...] = uk * (1.0 / (1.0 + jnp.exp(-e_ref[...].astype(jnp.float32))))
    lk_ref[...] = -DECAY_SCALE / (1.0 + jnp.exp(-d_ref[...].astype(jnp.float32)))

    row = lax.broadcasted_iota(jnp.int32, (SPAN, SPAN), 0)
    col = lax.broadcasted_iota(jnp.int32, (SPAN, SPAN), 1)
    differ = row ^ col
    eye_span = jnp.where(differ == 0, 1.0, 0.0)
    running = jnp.where(row <= col, 1.0, 0.0).astype(jnp.bfloat16)
    eye = jnp.where(
        lax.broadcasted_iota(jnp.int32, (HEAD_DIM, HEAD_DIM), 0)
        == lax.broadcasted_iota(jnp.int32, (HEAD_DIM, HEAD_DIM), 1),
        1.0,
        0.0,
    )
    strict = (row < col, row > col)
    inclusive = (row <= col, row >= col)

    def body(step, carry):
        units = []
        for part in range(UNROLL):
            chunk = step * UNROLL + part
            lanes = pl.ds(pl.multiple_of(chunk * SPAN, SPAN), SPAN)
            q = q_ref[:, lanes].astype(jnp.float32)
            k = k_ref[:, lanes].astype(jnp.float32)
            v = v_ref[:, lanes]
            u, er, lk = uk_ref[:, lanes], er_ref[:, lanes], lk_ref[:, lanes]
            high = lk.astype(jnp.bfloat16)
            rest = lk - high.astype(jnp.float32)
            low = rest.astype(jnp.bfloat16)
            sums = mm(jnp.concatenate([high, low], axis=0), running)
            cum = sums[:HEAD_DIM] + sums[HEAD_DIM:]
            prior = cum - lk
            last = cum[:, SPAN - 1 :]
            to_prior, fade = jnp.exp(prior), jnp.exp(last - cum)
            up_f, up_b = jnp.exp(-cum), jnp.exp(prior - last)
            dec_ref[chunk] = jnp.sum(eye * jnp.exp(last), axis=0, keepdims=True)
            both = (
                (u * to_prior, q * jnp.exp(cum), k * up_f, er * up_f, k * fade, er * fade),
                (u * fade, q * jnp.exp(last - prior), k * up_b, er * up_b, k * to_prior, er * to_prior),
            )
            for way in (0, 1):
                units.append((chunk, lanes, way, v, both[way]))
        state = []
        for chunk, lanes, way, v, (ud, qd, ku, eu, kend, eend) in units:
            gram = mm_tn(
                jnp.concatenate([ku, eu], axis=1), jnp.concatenate([ud, qd], axis=1)
            )
            k_mix = jnp.where(strict[way], gram[:SPAN, :SPAN], 0.0).astype(jnp.bfloat16)
            k_read = jnp.where(inclusive[way], gram[:SPAN, SPAN:], 0.0).astype(jnp.bfloat16)
            e_mix = jnp.where(strict[way], gram[SPAN:, :SPAN], 0.0)
            e_read = jnp.where(inclusive[way], gram[SPAN:, SPAN:], 0.0).astype(jnp.bfloat16)
            inv = (eye_span - jnp.where(differ == 1, e_mix, 0.0)).astype(jnp.bfloat16)
            mixed = mm(v, jnp.concatenate([k_mix, k_read], axis=1))
            state.append([e_mix, inv, mixed, e_read])
        width = 2
        while width < SPAN:
            inside = (differ >= width) & (differ < 2 * width)
            halves = [mm(inv, jnp.where(inside, e_mix, 0.0)) for e_mix, inv, _, _ in state]
            for unit, half in zip(state, halves):
                unit[1] = (unit[1].astype(jnp.float32) - mm(half, unit[1])).astype(jnp.bfloat16)
            width *= 2
        for (chunk, lanes, way, v, (ud, qd, ku, eu, kend, eend)), (_, inv, mixed, e_read) in zip(
            units, state
        ):
            solved = mm(jnp.concatenate([ud, mixed[:, :SPAN]], axis=0), inv).astype(jnp.bfloat16)
            read = mm(solved, e_read)
            ends = mm_nt(solved, eend)
            qh = (qh_f_ref, qh_b_ref)[way]
            qh[:, lanes] = (qd - read[:HEAD_DIM]).astype(jnp.bfloat16)
            out = mixed[:, SPAN:] - read[HEAD_DIM:]
            if way == 0:
                oloc_ref[:, lanes] = out
            else:
                oloc_ref[:, lanes] += out
            z_ref[way, chunk] = ends[:HEAD_DIM].astype(jnp.bfloat16)
            b_ref[way, chunk] = mm_nt(v, kend) - ends[HEAD_DIM:]
        return carry

    lax.fori_loop(0, count // UNROLL, body, 0)

    start = jnp.concatenate([jnp.zeros_like(eye), eye], axis=0)
    carried = [start, start]
    for step in range(count):
        for way, qh in ((0, qh_f_ref), (1, qh_b_ref)):
            chunk = step if way == 0 else count - 1 - step
            lanes = slice(chunk * SPAN, (chunk + 1) * SPAN)
            now = carried[way]
            narrow = now.astype(jnp.bfloat16)
            read = mm(narrow, qh[:, lanes])
            oloc_ref[:, lanes] += read[:HEAD_DIM]
            qp_ref[way * HEAD_DIM : (way + 1) * HEAD_DIM, lanes] = read[HEAD_DIM:].astype(jnp.bfloat16)
            moved = now * dec_ref[chunk] - mm(narrow, z_ref[way, chunk])
            carried[way] = jnp.concatenate(
                [moved[:HEAD_DIM] + b_ref[way, chunk], moved[HEAD_DIM:]], axis=0
            )
    for way in (0, 1):
        maps_ref[way] = jnp.concatenate(
            [carried[way][:HEAD_DIM], carried[way][HEAD_DIM:] - eye], axis=1
        ).astype(jnp.bfloat16)


def local_half(query, key, value, erase, decay):
    tokens = query.shape[1]
    count = tokens // SPAN
    full = lambda kind: jax.ShapeDtypeStruct((HEAD_DIM, tokens), kind)
    whole = lambda kind: pltpu.VMEM((HEAD_DIM, tokens), kind)
    return pl.pallas_call(
        local_kernel,
        out_shape=(
            full(jnp.float32),
            jax.ShapeDtypeStruct((2 * HEAD_DIM, tokens), jnp.bfloat16),
            jax.ShapeDtypeStruct((2, HEAD_DIM, 2 * HEAD_DIM), jnp.bfloat16),
        ),
        scratch_shapes=[
            whole(jnp.float32),
            whole(jnp.float32),
            whole(jnp.float32),
            whole(jnp.bfloat16),
            whole(jnp.bfloat16),
            pltpu.VMEM((2, count, HEAD_DIM, HEAD_DIM), jnp.bfloat16),
            pltpu.VMEM((2, count, HEAD_DIM, HEAD_DIM), jnp.float32),
            pltpu.VMEM((count, 1, HEAD_DIM), jnp.float32),
        ],
        cost_estimate=pl.CostEstimate(
            flops=16 * 22 * 2 * 128**3, bytes_accessed=tokens * 64 * 18, transcendentals=tokens * 64 * 9
        ),
        compiler_params=pltpu.CompilerParams(vmem_limit_bytes=16 * 2**20),
        name="mixer_local",
    )(query, key, value, erase, decay)


def stacked(wide):
    left = lax.broadcasted_iota(jnp.int32, (2 * HEAD_DIM, 2 * HEAD_DIM), 1) < HEAD_DIM
    full = wide.astype(jnp.float32)
    return jnp.where(left, jnp.concatenate([pltpu.roll(full, HEAD_DIM, 1), full], axis=0), 0.0)


def widened(tall):
    return tall[HEAD_DIM:] + pltpu.roll(tall[:HEAD_DIM], HEAD_DIM, 1)


def composed(first, later):
    return first + mm(first, later) + later


def step_kernel(upper_ref, arrived_ref, through_ref, past_ref, next_past_ref, next_through_ref):
    upper = upper_ref[0] != 0
    other = [stacked(arrived_ref[way]) for way in (0, 1)]
    mine = [stacked(through_ref[way]) for way in (0, 1)]
    near = jnp.where(upper, past_ref[0], past_ref[1])
    met = widened(composed(jnp.where(upper, other[0], other[1]), stacked(near)))
    next_past_ref[0] = jnp.where(upper, met, past_ref[0])
    next_past_ref[1] = jnp.where(upper, past_ref[1], met)
    for way in (0, 1):
        other_first = upper if way == 0 else jnp.logical_not(upper)
        first = jnp.where(other_first, other[way], mine[way])
        later = jnp.where(other_first, mine[way], other[way])
        next_through_ref[way] = widened(composed(first, later)).astype(jnp.bfloat16)


def in_vmem(count, scalars):
    return [pl.BlockSpec(memory_space=pltpu.SMEM)] * scalars + [
        pl.BlockSpec(memory_space=pltpu.VMEM)
    ] * count


def scan_step(upper, arrived, through, past):
    return pl.pallas_call(
        step_kernel,
        out_shape=(
            jax.ShapeDtypeStruct(past.shape, jnp.float32),
            jax.ShapeDtypeStruct(past.shape, jnp.bfloat16),
        ),
        in_specs=in_vmem(3, 1),
        out_specs=tuple(in_vmem(2, 0)),
        cost_estimate=pl.CostEstimate(
            flops=6 * 128**3, bytes_accessed=6 * 2 * past.size, transcendentals=0
        ),
        compiler_params=pltpu.CompilerParams(vmem_limit_bytes=4 * 2**20),
        name="scan_step",
    )(upper, arrived, through, past)


def finish_kernel(upper_ref, arrived_ref, past_ref, oloc_ref, qp_ref, gain_ref, out_ref):
    upper = upper_ref[0] != 0
    other = jnp.where(upper, arrived_ref[0].astype(jnp.float32), arrived_ref[1].astype(jnp.float32))
    near = jnp.where(upper, past_ref[0], past_ref[1])
    met = composed(stacked(other), stacked(near))[HEAD_DIM:]
    kept = stacked(jnp.where(upper, past_ref[1], past_ref[0]))[HEAD_DIM:]
    ahead, behind = jnp.where(upper, met, kept), jnp.where(upper, kept, met)
    states = ahead + pltpu.roll(behind, HEAD_DIM, 1)
    summed = oloc_ref[...] + mm(states, qp_ref[...])
    center = jnp.mean(summed, axis=0, keepdims=True)
    away = summed - center
    spread = jnp.mean(away * away, axis=0, keepdims=True)
    out_ref[...] = (
        away * lax.rsqrt(spread + HEAD_DIM * 1e-05) * gain_ref[...]
    ).astype(jnp.bfloat16)


def finish_half(upper, arrived, past, oloc, qp, gain):
    return pl.pallas_call(
        finish_kernel,
        out_shape=jax.ShapeDtypeStruct(oloc.shape, jnp.bfloat16),
        in_specs=in_vmem(5, 1),
        out_specs=in_vmem(1, 0)[0],
        cost_estimate=pl.CostEstimate(
            flops=4 * 128**3 + 16 * 128**3, bytes_accessed=2**20, transcendentals=1024
        ),
        compiler_params=pltpu.CompilerParams(vmem_limit_bytes=8 * 2**20),
        name="mixer_finish",
    )(upper, arrived, past, oloc, qp, gain)


def swapped(through, distance):
    count = lax.axis_size("ep")
    return lax.ppermute(through, "ep", [(i, i ^ distance) for i in range(count)])


def side(distance):
    return (lax.axis_index("ep") & distance).reshape(1).astype(jnp.int32)


def expert_kernel(rows_ref, gate_ref, up_ref, down_ref, out_ref):
    parts = rows_ref.shape[0]
    rows = jnp.concatenate([rows_ref[j] for j in range(parts)], axis=1)
    gate = mm(rows, gate_ref[...])
    up = mm(rows, up_ref[...])
    hidden = (gate / (1.0 + jnp.exp(-gate)) * up).astype(jnp.bfloat16)
    result = mm(hidden, down_ref[...]).astype(jnp.bfloat16)
    for j in range(parts):
        out_ref[j] = result[:, j * LANES : (j + 1) * LANES]


def expert_rows(rows, gate, up, down):
    parts, total, lanes = rows.shape
    tile = 256 if total % 256 == 0 else total
    block = pl.BlockSpec((parts, tile, lanes), lambda i: (0, i, 0))
    fixed = lambda array: pl.BlockSpec(array.shape, lambda i: (0, 0))
    return pl.pallas_call(
        expert_kernel,
        grid=(total // tile,),
        in_specs=[block, fixed(gate), fixed(up), fixed(down)],
        out_specs=block,
        out_shape=jax.ShapeDtypeStruct(rows.shape, jnp.bfloat16),
        cost_estimate=pl.CostEstimate(
            flops=6 * total * gate.size,
            bytes_accessed=2 * (2 * rows.size + 3 * gate.size),
            transcendentals=total * gate.shape[1],
        ),
        compiler_params=pltpu.CompilerParams(vmem_limit_bytes=63600000),
        name="expert_rows",
    )(rows, gate, up, down)


def slot_targets(routes, experts_n, capacity):
    onehot = (routes[:, :, None] == jnp.arange(experts_n, dtype=jnp.int32)[None, None, :]).astype(
        jnp.int32
    )
    flat = onehot.reshape(-1, experts_n)
    before = jnp.cumsum(flat, axis=0) - flat
    slot_index = jnp.sum(before * flat, axis=-1).reshape(routes.shape)
    return routes * capacity + slot_index


def dispatch_matrix(targets, slot_total):
    matches = targets[None, :, :] == jnp.arange(slot_total, dtype=jnp.int32)[:, None, None]
    return jnp.sum(matches.astype(jnp.float32), axis=-1).astype(jnp.bfloat16)


def spread(array, axis):
    return lax.all_to_all(array, axis, 0, 0, tiled=True)


def on_device(
    query_in,
    key_in,
    value_in,
    erase_pre,
    decay_pre,
    mix_gain,
    expert_in,
    expert_gain,
    routes,
    route_weight,
    gate_weight,
    up_weight,
    down_weight,
):
    experts_n, shares = lax.axis_size("ep"), lax.axis_size("tp")
    row_count, features = expert_in.shape
    capacity = 3 * routes.shape[1] * row_count // (2 * experts_n)
    slot_total = experts_n * capacity
    col_count = features // shares
    at = lax.axis_index("tp") * col_count
    input_f = expert_in.astype(jnp.float32)
    scale = lax.rsqrt(jnp.mean(input_f * input_f, axis=-1, keepdims=True) + 1e-06)
    own = lax.dynamic_slice_in_dim(expert_in, at, col_count, 1).astype(jnp.float32)
    normed = (own * scale * lax.dynamic_slice_in_dim(expert_gain, at, col_count, 0)).astype(
        jnp.bfloat16
    )
    targets = slot_targets(routes, experts_n, capacity)
    outgoing = mm(dispatch_matrix(targets, slot_total), normed).astype(jnp.bfloat16)
    arrived = spread(outgoing.reshape(experts_n, capacity, col_count), "ep").reshape(
        slot_total, col_count
    )
    oloc, qp, own_maps = local_half(query_in, key_in, value_in, erase_pre, decay_pre)
    arrived, own_maps = lax.optimization_barrier((arrived, own_maps))
    shared = spread(jnp.broadcast_to(arrived[None], (shares, *arrived.shape)), "tp")

    past, through, distance = jnp.zeros(own_maps.shape, jnp.float32), own_maps, 1
    while distance < experts_n // 4:
        past, through = scan_step(side(distance), swapped(through, distance), through, past)
        distance *= 2
    shared, past, through = lax.optimization_barrier((shared, past, through))
    partial = expert_rows(shared, gate_weight[0], up_weight[0], down_weight[0])
    partial, past, through = lax.optimization_barrier((partial, past, through))
    while distance < experts_n // 2:
        past, through = scan_step(side(distance), swapped(through, distance), through, past)
        distance *= 2
    crossing = swapped(through, distance)
    pieces = spread(partial, "tp")
    pieces, crossing = lax.optimization_barrier((pieces, crossing))
    summed = jnp.sum(pieces.astype(jnp.float32), axis=0).astype(jnp.bfloat16)
    returned = spread(summed.reshape(experts_n, capacity, col_count), "ep").reshape(
        slot_total, col_count
    )
    mixer_out = finish_half(side(distance), crossing, past, oloc, qp, mix_gain[:, None])
    matches = targets[:, :, None] == jnp.arange(slot_total, dtype=jnp.int32)[None, None, :]
    combine = jnp.sum(matches.astype(jnp.float32) * route_weight[:, :, None], axis=1)
    expert_out = jnp.dot(combine, returned.astype(jnp.float32)).astype(jnp.bfloat16)
    return (mixer_out, expert_out)


def solution(mesh):
    placed = (
        P("tp", "ep"),
        P("tp", "ep"),
        P("tp", "ep"),
        P("tp", "ep"),
        P("tp", "ep"),
        P("tp"),
        P("ep", None),
        P(),
        P("ep", None),
        P("ep", None),
        P("ep", None, "tp"),
        P("ep", None, "tp"),
        P("ep", "tp", None),
    )
    return jax.shard_map(
        on_device,
        mesh=mesh,
        in_specs=placed,
        out_specs=(P("tp", "ep"), P("ep", "tp")),
        check_vma=False,
    )
```

```python
import functools

import jax
import jax.numpy as jnp
from jax import lax
from jax.experimental import pallas as pl
from jax.experimental.pallas import tpu as pltpu
from jax.sharding import PartitionSpec as P

HEAD_DIM = 64
LANES = 128
SPAN = 128
UNROLL = 2
DECAY_SCALE = 0.6065306597126334


def mm(a, b):
    return jnp.dot(
        a.astype(jnp.bfloat16), b.astype(jnp.bfloat16), preferred_element_type=jnp.float32
    )


def mm_tn(a, b):
    return lax.dot_general(
        a.astype(jnp.bfloat16),
        b.astype(jnp.bfloat16),
        (((0,), (0,)), ((), ())),
        preferred_element_type=jnp.float32,
    )


def mm_nt(a, b):
    return lax.dot_general(
        a.astype(jnp.bfloat16),
        b.astype(jnp.bfloat16),
        (((1,), (1,)), ((), ())),
        preferred_element_type=jnp.float32,
    )


def local_kernel(
    q_ref, k_ref, v_ref, e_ref, d_ref, oloc_ref, qp_ref, maps_ref,
    uk_ref, er_ref, lk_ref, qh_f_ref, qh_b_ref, z_ref, b_ref, dec_ref,
):
    count = q_ref.shape[1] // SPAN
    kf = k_ref[...].astype(jnp.float32)
    uk = kf * lax.rsqrt(jnp.sum(kf * kf, axis=0, keepdims=True) + 1e-05)
    uk_ref[...] = uk
    er_ref[...] = uk * (1.0 / (1.0 + jnp.exp(-e_ref[...].astype(jnp.float32))))
    lk_ref[...] = -DECAY_SCALE / (1.0 + jnp.exp(-d_ref[...].astype(jnp.float32)))

    row = lax.broadcasted_iota(jnp.int32, (SPAN, SPAN), 0)
    col = lax.broadcasted_iota(jnp.int32, (SPAN, SPAN), 1)
    differ = row ^ col
    eye_span = jnp.where(differ == 0, 1.0, 0.0)
    running = jnp.where(row <= col, 1.0, 0.0).astype(jnp.bfloat16)
    eye = jnp.where(
        lax.broadcasted_iota(jnp.int32, (HEAD_DIM, HEAD_DIM), 0)
        == lax.broadcasted_iota(jnp.int32, (HEAD_DIM, HEAD_DIM), 1),
        1.0,
        0.0,
    )
    strict = (row < col, row > col)
    inclusive = (row <= col, row >= col)

    def body(step, carry):
        units = []
        for part in range(UNROLL):
            chunk = step * UNROLL + part
            lanes = pl.ds(pl.multiple_of(chunk * SPAN, SPAN), SPAN)
            q = q_ref[:, lanes].astype(jnp.float32)
            k = k_ref[:, lanes].astype(jnp.float32)
            v = v_ref[:, lanes]
            u, er, lk = uk_ref[:, lanes], er_ref[:, lanes], lk_ref[:, lanes]
            high = lk.astype(jnp.bfloat16)
            rest = lk - high.astype(jnp.float32)
            low = rest.astype(jnp.bfloat16)
            sums = mm(jnp.concatenate([high, low], axis=0), running)
            cum = sums[:HEAD_DIM] + sums[HEAD_DIM:]
            prior = cum - lk
            last = cum[:, SPAN - 1 :]
            to_prior, fade = jnp.exp(prior), jnp.exp(last - cum)
            up_f, up_b = jnp.exp(-cum), jnp.exp(prior - last)
            dec_ref[chunk] = jnp.sum(eye * jnp.exp(last), axis=0, keepdims=True)
            both = (
                (u * to_prior, q * jnp.exp(cum), k * up_f, er * up_f, k * fade, er * fade),
                (u * fade, q * jnp.exp(last - prior), k * up_b, er * up_b, k * to_prior, er * to_prior),
            )
            for way in (0, 1):
                units.append((chunk, lanes, way, v, both[way]))
        state = []
        for chunk, lanes, way, v, (ud, qd, ku, eu, kend, eend) in units:
            gram = mm_tn(
                jnp.concatenate([ku, eu], axis=1), jnp.concatenate([ud, qd], axis=1)
            )
            k_mix = jnp.where(strict[way], gram[:SPAN, :SPAN], 0.0).astype(jnp.bfloat16)
            k_read = jnp.where(inclusive[way], gram[:SPAN, SPAN:], 0.0).astype(jnp.bfloat16)
            e_mix = jnp.where(strict[way], gram[SPAN:, :SPAN], 0.0)
            e_read = jnp.where(inclusive[way], gram[SPAN:, SPAN:], 0.0).astype(jnp.bfloat16)
            inv = (eye_span - jnp.where(differ == 1, e_mix, 0.0)).astype(jnp.bfloat16)
            mixed = mm(v, jnp.concatenate([k_mix, k_read], axis=1))
            state.append([e_mix, inv, mixed, e_read])
        width = 2
        while width < SPAN:
            inside = (differ >= width) & (differ < 2 * width)
            halves = [mm(inv, jnp.where(inside, e_mix, 0.0)) for e_mix, inv, _, _ in state]
            for unit, half in zip(state, halves):
                unit[1] = (unit[1].astype(jnp.float32) - mm(half, unit[1])).astype(jnp.bfloat16)
            width *= 2
        for (chunk, lanes, way, v, (ud, qd, ku, eu, kend, eend)), (_, inv, mixed, e_read) in zip(
            units, state
        ):
            solved = mm(jnp.concatenate([ud, mixed[:, :SPAN]], axis=0), inv).astype(jnp.bfloat16)
            read = mm(solved, e_read)
            ends = mm_nt(solved, eend)
            qh = (qh_f_ref, qh_b_ref)[way]
            qh[:, lanes] = (qd - read[:HEAD_DIM]).astype(jnp.bfloat16)
            out = mixed[:, SPAN:] - read[HEAD_DIM:]
            if way == 0:
                oloc_ref[:, lanes] = out
            else:
                oloc_ref[:, lanes] += out
            z_ref[way, chunk] = ends[:HEAD_DIM].astype(jnp.bfloat16)
            b_ref[way, chunk] = mm_nt(v, kend) - ends[HEAD_DIM:]
        return carry

    lax.fori_loop(0, count // UNROLL, body, 0)

    start = jnp.concatenate([jnp.zeros_like(eye), eye], axis=0)
    carried = [start, start]
    for step in range(count):
        for way, qh in ((0, qh_f_ref), (1, qh_b_ref)):
            chunk = step if way == 0 else count - 1 - step
            lanes = slice(chunk * SPAN, (chunk + 1) * SPAN)
            now = carried[way]
            narrow = now.astype(jnp.bfloat16)
            read = mm(narrow, qh[:, lanes])
            oloc_ref[:, lanes] += read[:HEAD_DIM]
            qp_ref[way * HEAD_DIM : (way + 1) * HEAD_DIM, lanes] = read[HEAD_DIM:].astype(jnp.bfloat16)
            moved = now * dec_ref[chunk] - mm(narrow, z_ref[way, chunk])
            carried[way] = jnp.concatenate(
                [moved[:HEAD_DIM] + b_ref[way, chunk], moved[HEAD_DIM:]], axis=0
            )
    for way in (0, 1):
        maps_ref[way] = jnp.concatenate(
            [carried[way][:HEAD_DIM], carried[way][HEAD_DIM:] - eye], axis=1
        ).astype(jnp.bfloat16)


def local_half(query, key, value, erase, decay):
    tokens = query.shape[1]
    count = tokens // SPAN
    full = lambda kind: jax.ShapeDtypeStruct((HEAD_DIM, tokens), kind)
    whole = lambda kind: pltpu.VMEM((HEAD_DIM, tokens), kind)
    return pl.pallas_call(
        local_kernel,
        out_shape=(
            full(jnp.float32),
            jax.ShapeDtypeStruct((2 * HEAD_DIM, tokens), jnp.bfloat16),
            jax.ShapeDtypeStruct((2, HEAD_DIM, 2 * HEAD_DIM), jnp.bfloat16),
        ),
        scratch_shapes=[
            whole(jnp.float32),
            whole(jnp.float32),
            whole(jnp.float32),
            whole(jnp.bfloat16),
            whole(jnp.bfloat16),
            pltpu.VMEM((2, count, HEAD_DIM, HEAD_DIM), jnp.bfloat16),
            pltpu.VMEM((2, count, HEAD_DIM, HEAD_DIM), jnp.float32),
            pltpu.VMEM((count, 1, HEAD_DIM), jnp.float32),
        ],
        cost_estimate=pl.CostEstimate(
            flops=16 * 22 * 2 * 128**3, bytes_accessed=tokens * 64 * 18, transcendentals=tokens * 64 * 9
        ),
        compiler_params=pltpu.CompilerParams(vmem_limit_bytes=16 * 2**20),
        name="mixer_local",
    )(query, key, value, erase, decay)


def stacked(wide):
    left = lax.broadcasted_iota(jnp.int32, (2 * HEAD_DIM, 2 * HEAD_DIM), 1) < HEAD_DIM
    full = wide.astype(jnp.float32)
    return jnp.where(left, jnp.concatenate([pltpu.roll(full, HEAD_DIM, 1), full], axis=0), 0.0)


def widened(tall):
    return tall[HEAD_DIM:] + pltpu.roll(tall[:HEAD_DIM], HEAD_DIM, 1)


def composed(first, later):
    return first + mm(first, later) + later


def step_kernel(upper_ref, arrived_ref, through_ref, past_ref, next_past_ref, next_through_ref):
    upper = upper_ref[0] != 0
    other = [stacked(arrived_ref[way]) for way in (0, 1)]
    mine = [stacked(through_ref[way]) for way in (0, 1)]
    near = jnp.where(upper, past_ref[0], past_ref[1])
    met = widened(composed(jnp.where(upper, other[0], other[1]), stacked(near)))
    next_past_ref[0] = jnp.where(upper, met, past_ref[0])
    next_past_ref[1] = jnp.where(upper, past_ref[1], met)
    for way in (0, 1):
        other_first = upper if way == 0 else jnp.logical_not(upper)
        first = jnp.where(other_first, other[way], mine[way])
        later = jnp.where(other_first, mine[way], other[way])
        next_through_ref[way] = widened(composed(first, later)).astype(jnp.bfloat16)


def in_vmem(count, scalars):
    return [pl.BlockSpec(memory_space=pltpu.SMEM)] * scalars + [
        pl.BlockSpec(memory_space=pltpu.VMEM)
    ] * count


def scan_step(upper, arrived, through, past):
    return pl.pallas_call(
        step_kernel,
        out_shape=(
            jax.ShapeDtypeStruct(past.shape, jnp.float32),
            jax.ShapeDtypeStruct(past.shape, jnp.bfloat16),
        ),
        in_specs=in_vmem(3, 1),
        out_specs=tuple(in_vmem(2, 0)),
        cost_estimate=pl.CostEstimate(
            flops=6 * 128**3, bytes_accessed=6 * 2 * past.size, transcendentals=0
        ),
        compiler_params=pltpu.CompilerParams(vmem_limit_bytes=4 * 2**20),
        name="scan_step",
    )(upper, arrived, through, past)


def finish_kernel(upper_ref, arrived_ref, past_ref, oloc_ref, qp_ref, gain_ref, out_ref):
    upper = upper_ref[0] != 0
    other = jnp.where(upper, arrived_ref[0].astype(jnp.float32), arrived_ref[1].astype(jnp.float32))
    near = jnp.where(upper, past_ref[0], past_ref[1])
    met = composed(stacked(other), stacked(near))[HEAD_DIM:]
    kept = stacked(jnp.where(upper, past_ref[1], past_ref[0]))[HEAD_DIM:]
    ahead, behind = jnp.where(upper, met, kept), jnp.where(upper, kept, met)
    states = ahead + pltpu.roll(behind, HEAD_DIM, 1)
    summed = oloc_ref[...] + mm(states, qp_ref[...])
    center = jnp.mean(summed, axis=0, keepdims=True)
    away = summed - center
    spread = jnp.mean(away * away, axis=0, keepdims=True)
    out_ref[...] = (
        away * lax.rsqrt(spread + HEAD_DIM * 1e-05) * gain_ref[...]
    ).astype(jnp.bfloat16)


def finish_half(upper, arrived, past, oloc, qp, gain):
    return pl.pallas_call(
        finish_kernel,
        out_shape=jax.ShapeDtypeStruct(oloc.shape, jnp.bfloat16),
        in_specs=in_vmem(5, 1),
        out_specs=in_vmem(1, 0)[0],
        cost_estimate=pl.CostEstimate(
            flops=4 * 128**3 + 16 * 128**3, bytes_accessed=2**20, transcendentals=1024
        ),
        compiler_params=pltpu.CompilerParams(vmem_limit_bytes=8 * 2**20),
        name="mixer_finish",
    )(upper, arrived, past, oloc, qp, gain)


def swapped(through, distance):
    count = lax.axis_size("ep")
    return lax.ppermute(through, "ep", [(i, i ^ distance) for i in range(count)])


def side(distance):
    return (lax.axis_index("ep") & distance).reshape(1).astype(jnp.int32)


def expert_kernel(rows_ref, gate_ref, up_ref, down_ref, out_ref):
    parts = rows_ref.shape[0]
    rows = jnp.concatenate([rows_ref[j] for j in range(parts)], axis=1)
    gate = mm(rows, gate_ref[...])
    up = mm(rows, up_ref[...])
    hidden = (gate / (1.0 + jnp.exp(-gate)) * up).astype(jnp.bfloat16)
    result = mm(hidden, down_ref[...]).astype(jnp.bfloat16)
    for j in range(parts):
        out_ref[j] = result[:, j * LANES : (j + 1) * LANES]


def expert_rows(rows, gate, up, down):
    parts, total, lanes = rows.shape
    tile = 128 if total % 128 == 0 else total
    block = pl.BlockSpec((parts, tile, lanes), lambda i: (0, i, 0))
    fixed = lambda array: pl.BlockSpec(array.shape, lambda i: (0, 0))
    return pl.pallas_call(
        expert_kernel,
        grid=(total // tile,),
        in_specs=[block, fixed(gate), fixed(up), fixed(down)],
        out_specs=block,
        out_shape=jax.ShapeDtypeStruct(rows.shape, jnp.bfloat16),
        cost_estimate=pl.CostEstimate(
            flops=6 * total * gate.size,
            bytes_accessed=2 * (2 * rows.size + 3 * gate.size),
            transcendentals=total * gate.shape[1],
        ),
        compiler_params=pltpu.CompilerParams(vmem_limit_bytes=63600000),
        name="expert_rows",
    )(rows, gate, up, down)


def route_kernel(
    capacity, at_ref, rows_ref, gain_ref, routes_ref, weight_ref, outgoing_ref, combine_ref
):
    total, slots = combine_ref.shape
    full = rows_ref[...].astype(jnp.float32)
    scale = lax.rsqrt(jnp.mean(full * full, axis=1, keepdims=True) + 1e-06)
    lanes = pl.ds(pl.multiple_of(at_ref[0], LANES), LANES)
    normed = rows_ref[:, lanes].astype(jnp.float32) * scale * gain_ref[:, lanes]
    expert = lax.broadcasted_iota(jnp.int32, (total, LANES), 1)
    named = [
        jnp.where(routes_ref[:, k : k + 1] == expert, 1.0, 0.0)
        for k in range(routes_ref.shape[1])
    ]
    earlier = lax.broadcasted_iota(jnp.int32, (total, total), 0) > lax.broadcasted_iota(
        jnp.int32, (total, total), 1
    )
    before = mm(jnp.where(earlier, 1.0, 0.0), sum(named))
    slot = lax.broadcasted_iota(jnp.int32, (total, slots), 1)
    chosen = jnp.zeros((total, slots), jnp.float32)
    combine = jnp.zeros((total, slots), jnp.float32)
    for k, one in enumerate(named):
        place = jnp.sum(before * one, axis=1, keepdims=True).astype(jnp.int32)
        hit = routes_ref[:, k : k + 1] * capacity + place == slot
        chosen = jnp.where(hit, 1.0, chosen)
        combine = jnp.where(hit, weight_ref[:, k : k + 1], combine)
    outgoing_ref[...] = mm_tn(chosen, normed).astype(jnp.bfloat16)
    combine_ref[...] = combine.astype(jnp.bfloat16)


def routed(at, rows, gain, routes, weight, slots, capacity):
    total = rows.shape[0]
    return pl.pallas_call(
        functools.partial(route_kernel, capacity),
        out_shape=(
            jax.ShapeDtypeStruct((slots, LANES), jnp.bfloat16),
            jax.ShapeDtypeStruct((total, slots), jnp.bfloat16),
        ),
        in_specs=in_vmem(4, 1),
        out_specs=tuple(in_vmem(2, 0)),
        cost_estimate=pl.CostEstimate(
            flops=4 * total * slots * LANES, bytes_accessed=2 * rows.size, transcendentals=total
        ),
        compiler_params=pltpu.CompilerParams(vmem_limit_bytes=24 * 2**20),
        name="route_rows",
    )(at, rows, gain, routes, weight)


def sum_kernel(pieces_ref, out_ref):
    total = pieces_ref[0].astype(jnp.float32)
    for j in range(1, pieces_ref.shape[0]):
        total += pieces_ref[j].astype(jnp.float32)
    out_ref[...] = total.astype(jnp.bfloat16)


def summed_pieces(pieces):
    parts, total, lanes = pieces.shape
    tile = 128 if total % 128 == 0 else total
    return pl.pallas_call(
        sum_kernel,
        grid=(total // tile,),
        in_specs=[pl.BlockSpec((parts, tile, lanes), lambda i: (0, i, 0))],
        out_specs=pl.BlockSpec((tile, lanes), lambda i: (i, 0)),
        out_shape=jax.ShapeDtypeStruct((total, lanes), jnp.bfloat16),
        cost_estimate=pl.CostEstimate(
            flops=pieces.size, bytes_accessed=2 * pieces.size, transcendentals=0
        ),
        compiler_params=pltpu.CompilerParams(vmem_limit_bytes=63600000),
        name="sum_pieces",
    )(pieces)


def spread(array, axis):
    return lax.all_to_all(array, axis, 0, 0, tiled=True)


def on_device(
    query_in,
    key_in,
    value_in,
    erase_pre,
    decay_pre,
    mix_gain,
    expert_in,
    expert_gain,
    routes,
    route_weight,
    gate_weight,
    up_weight,
    down_weight,
):
    experts_n, shares = lax.axis_size("ep"), lax.axis_size("tp")
    row_count, features = expert_in.shape
    capacity = 3 * routes.shape[1] * row_count // (2 * experts_n)
    slot_total = experts_n * capacity
    col_count = features // shares
    at = lax.axis_index("tp") * col_count
    outgoing, combine = routed(
        at.reshape(1).astype(jnp.int32),
        expert_in,
        expert_gain[None],
        routes,
        route_weight,
        slot_total,
        capacity,
    )
    arrived = spread(outgoing.reshape(experts_n, capacity, col_count), "ep").reshape(
        slot_total, col_count
    )
    arrived, query_in = lax.optimization_barrier((arrived, query_in))
    oloc, qp, own_maps = local_half(query_in, key_in, value_in, erase_pre, decay_pre)
    shared = spread(jnp.broadcast_to(arrived[None], (shares, *arrived.shape)), "tp")

    past, through, distance = jnp.zeros(own_maps.shape, jnp.float32), own_maps, 1
    while distance < experts_n // 4:
        past, through = scan_step(side(distance), swapped(through, distance), through, past)
        distance *= 2
    shared, past, through = lax.optimization_barrier((shared, past, through))
    partial = expert_rows(shared, gate_weight[0], up_weight[0], down_weight[0])
    partial, past, through = lax.optimization_barrier((partial, past, through))
    while distance < experts_n // 2:
        past, through = scan_step(side(distance), swapped(through, distance), through, past)
        distance *= 2
    crossing = swapped(through, distance)
    pieces = spread(partial, "tp")
    pieces, crossing = lax.optimization_barrier((pieces, crossing))
    summed = summed_pieces(pieces)
    returned = spread(summed.reshape(experts_n, capacity, col_count), "ep").reshape(
        slot_total, col_count
    )
    mixer_out = finish_half(side(distance), crossing, past, oloc, qp, mix_gain[:, None])
    expert_out = mm(combine, returned).astype(jnp.bfloat16)
    return (mixer_out, expert_out)


def solution(mesh):
    placed = (
        P("tp", "ep"),
        P("tp", "ep"),
        P("tp", "ep"),
        P("tp", "ep"),
        P("tp", "ep"),
        P("tp"),
        P("ep", None),
        P(),
        P("ep", None),
        P("ep", None),
        P("ep", None, "tp"),
        P("ep", None, "tp"),
        P("ep", "tp", None),
    )
    return jax.shard_map(
        on_device,
        mesh=mesh,
        in_specs=placed,
        out_specs=(P("tp", "ep"), P("ep", "tp")),
        check_vma=False,
    )
```

```python
import functools

import jax
import jax.numpy as jnp
from jax import lax
from jax.experimental import pallas as pl
from jax.experimental.pallas import tpu as pltpu
from jax.sharding import PartitionSpec as P

HEAD_DIM = 64
LANES = 128
SPAN = 128
UNROLL = 2
DECAY_SCALE = 0.6065306597126334


def mm(a, b):
    return jnp.dot(
        a.astype(jnp.bfloat16), b.astype(jnp.bfloat16), preferred_element_type=jnp.float32
    )


def mm_tn(a, b):
    return lax.dot_general(
        a.astype(jnp.bfloat16),
        b.astype(jnp.bfloat16),
        (((0,), (0,)), ((), ())),
        preferred_element_type=jnp.float32,
    )


def mm_nt(a, b):
    return lax.dot_general(
        a.astype(jnp.bfloat16),
        b.astype(jnp.bfloat16),
        (((1,), (1,)), ((), ())),
        preferred_element_type=jnp.float32,
    )


def local_kernel(
    q_ref, k_ref, v_ref, e_ref, d_ref, oloc_ref, qp_ref, maps_ref,
    uk_ref, er_ref, lk_ref, qh_f_ref, qh_b_ref, z_ref, b_ref, dec_ref,
):
    count = q_ref.shape[1] // SPAN
    kf = k_ref[...].astype(jnp.float32)
    uk = kf * lax.rsqrt(jnp.sum(kf * kf, axis=0, keepdims=True) + 1e-05)
    uk_ref[...] = uk
    er_ref[...] = uk * (1.0 / (1.0 + jnp.exp(-e_ref[...].astype(jnp.float32))))
    lk_ref[...] = -DECAY_SCALE / (1.0 + jnp.exp(-d_ref[...].astype(jnp.float32)))

    row = lax.broadcasted_iota(jnp.int32, (SPAN, SPAN), 0)
    col = lax.broadcasted_iota(jnp.int32, (SPAN, SPAN), 1)
    differ = row ^ col
    eye_span = jnp.where(differ == 0, 1.0, 0.0)
    running = jnp.where(row <= col, 1.0, 0.0).astype(jnp.bfloat16)
    eye = jnp.where(
        lax.broadcasted_iota(jnp.int32, (HEAD_DIM, HEAD_DIM), 0)
        == lax.broadcasted_iota(jnp.int32, (HEAD_DIM, HEAD_DIM), 1),
        1.0,
        0.0,
    )
    strict = (row < col, row > col)
    inclusive = (row <= col, row >= col)

    def body(step, carry):
        units = []
        for part in range(UNROLL):
            chunk = step * UNROLL + part
            lanes = pl.ds(pl.multiple_of(chunk * SPAN, SPAN), SPAN)
            q = q_ref[:, lanes].astype(jnp.float32)
            k = k_ref[:, lanes].astype(jnp.float32)
            v = v_ref[:, lanes]
            u, er, lk = uk_ref[:, lanes], er_ref[:, lanes], lk_ref[:, lanes]
            high = lk.astype(jnp.bfloat16)
            rest = lk - high.astype(jnp.float32)
            low = rest.astype(jnp.bfloat16)
            sums = mm(jnp.concatenate([high, low], axis=0), running)
            cum = sums[:HEAD_DIM] + sums[HEAD_DIM:]
            prior = cum - lk
            last = cum[:, SPAN - 1 :]
            to_prior, fade = jnp.exp(prior), jnp.exp(last - cum)
            up_f, up_b = jnp.exp(-cum), jnp.exp(prior - last)
            dec_ref[chunk] = jnp.sum(eye * jnp.exp(last), axis=0, keepdims=True)
            both = (
                (u * to_prior, q * jnp.exp(cum), k * up_f, er * up_f, k * fade, er * fade),
                (u * fade, q * jnp.exp(last - prior), k * up_b, er * up_b, k * to_prior, er * to_prior),
            )
            for way in (0, 1):
                units.append((chunk, lanes, way, v, both[way]))
        state = []
        for chunk, lanes, way, v, (ud, qd, ku, eu, kend, eend) in units:
            gram = mm_tn(
                jnp.concatenate([ku, eu], axis=1), jnp.concatenate([ud, qd], axis=1)
            )
            k_mix = jnp.where(strict[way], gram[:SPAN, :SPAN], 0.0).astype(jnp.bfloat16)
            k_read = jnp.where(inclusive[way], gram[:SPAN, SPAN:], 0.0).astype(jnp.bfloat16)
            e_mix = jnp.where(strict[way], gram[SPAN:, :SPAN], 0.0)
            e_read = jnp.where(inclusive[way], gram[SPAN:, SPAN:], 0.0).astype(jnp.bfloat16)
            inv = (eye_span - jnp.where(differ == 1, e_mix, 0.0)).astype(jnp.bfloat16)
            mixed = mm(v, jnp.concatenate([k_mix, k_read], axis=1))
            state.append([e_mix, inv, mixed, e_read])
        width = 2
        while width < SPAN:
            inside = (differ >= width) & (differ < 2 * width)
            halves = [mm(inv, jnp.where(inside, e_mix, 0.0)) for e_mix, inv, _, _ in state]
            for unit, half in zip(state, halves):
                unit[1] = (unit[1].astype(jnp.float32) - mm(half, unit[1])).astype(jnp.bfloat16)
            width *= 2
        for (chunk, lanes, way, v, (ud, qd, ku, eu, kend, eend)), (_, inv, mixed, e_read) in zip(
            units, state
        ):
            solved = mm(jnp.concatenate([ud, mixed[:, :SPAN]], axis=0), inv).astype(jnp.bfloat16)
            read = mm(solved, e_read)
            ends = mm_nt(solved, eend)
            qh = (qh_f_ref, qh_b_ref)[way]
            qh[:, lanes] = (qd - read[:HEAD_DIM]).astype(jnp.bfloat16)
            out = mixed[:, SPAN:] - read[HEAD_DIM:]
            if way == 0:
                oloc_ref[:, lanes] = out
            else:
                oloc_ref[:, lanes] += out
            z_ref[way, chunk] = ends[:HEAD_DIM].astype(jnp.bfloat16)
            b_ref[way, chunk] = mm_nt(v, kend) - ends[HEAD_DIM:]
        return carry

    lax.fori_loop(0, count // UNROLL, body, 0)

    start = jnp.concatenate([jnp.zeros_like(eye), eye], axis=0)
    carried = [start, start]
    for step in range(count):
        for way, qh in ((0, qh_f_ref), (1, qh_b_ref)):
            chunk = step if way == 0 else count - 1 - step
            lanes = slice(chunk * SPAN, (chunk + 1) * SPAN)
            now = carried[way]
            narrow = now.astype(jnp.bfloat16)
            read = mm(narrow, qh[:, lanes])
            oloc_ref[:, lanes] += read[:HEAD_DIM]
            qp_ref[way * HEAD_DIM : (way + 1) * HEAD_DIM, lanes] = read[HEAD_DIM:].astype(jnp.bfloat16)
            moved = now * dec_ref[chunk] - mm(narrow, z_ref[way, chunk])
            carried[way] = jnp.concatenate(
                [moved[:HEAD_DIM] + b_ref[way, chunk], moved[HEAD_DIM:]], axis=0
            )
    for way in (0, 1):
        maps_ref[way] = jnp.concatenate(
            [carried[way][:HEAD_DIM], carried[way][HEAD_DIM:] - eye], axis=1
        ).astype(jnp.bfloat16)


def local_half(query, key, value, erase, decay):
    tokens = query.shape[1]
    count = tokens // SPAN
    full = lambda kind: jax.ShapeDtypeStruct((HEAD_DIM, tokens), kind)
    whole = lambda kind: pltpu.VMEM((HEAD_DIM, tokens), kind)
    return pl.pallas_call(
        local_kernel,
        out_shape=(
            full(jnp.float32),
            jax.ShapeDtypeStruct((2 * HEAD_DIM, tokens), jnp.bfloat16),
            jax.ShapeDtypeStruct((2, HEAD_DIM, 2 * HEAD_DIM), jnp.bfloat16),
        ),
        scratch_shapes=[
            whole(jnp.float32),
            whole(jnp.float32),
            whole(jnp.float32),
            whole(jnp.bfloat16),
            whole(jnp.bfloat16),
            pltpu.VMEM((2, count, HEAD_DIM, HEAD_DIM), jnp.bfloat16),
            pltpu.VMEM((2, count, HEAD_DIM, HEAD_DIM), jnp.float32),
            pltpu.VMEM((count, 1, HEAD_DIM), jnp.float32),
        ],
        cost_estimate=pl.CostEstimate(
            flops=16 * 22 * 2 * 128**3, bytes_accessed=tokens * 64 * 18, transcendentals=tokens * 64 * 9
        ),
        compiler_params=pltpu.CompilerParams(vmem_limit_bytes=66000000),
        name="mixer_local",
    )(query, key, value, erase, decay)


def stacked(wide):
    left = lax.broadcasted_iota(jnp.int32, (2 * HEAD_DIM, 2 * HEAD_DIM), 1) < HEAD_DIM
    full = wide.astype(jnp.float32)
    return jnp.where(left, jnp.concatenate([pltpu.roll(full, HEAD_DIM, 1), full], axis=0), 0.0)


def widened(tall):
    return tall[HEAD_DIM:] + pltpu.roll(tall[:HEAD_DIM], HEAD_DIM, 1)


def composed(first, later):
    return first + mm(first, later) + later


def step_kernel(upper_ref, arrived_ref, through_ref, past_ref, next_past_ref, next_through_ref):
    upper = upper_ref[0] != 0
    other = [stacked(arrived_ref[way]) for way in (0, 1)]
    mine = [stacked(through_ref[way]) for way in (0, 1)]
    near = jnp.where(upper, past_ref[0], past_ref[1])
    met = widened(composed(jnp.where(upper, other[0], other[1]), stacked(near)))
    next_past_ref[0] = jnp.where(upper, met, past_ref[0])
    next_past_ref[1] = jnp.where(upper, past_ref[1], met)
    for way in (0, 1):
        other_first = upper if way == 0 else jnp.logical_not(upper)
        first = jnp.where(other_first, other[way], mine[way])
        later = jnp.where(other_first, mine[way], other[way])
        next_through_ref[way] = widened(composed(first, later)).astype(jnp.bfloat16)


def in_vmem(count, scalars):
    return [pl.BlockSpec(memory_space=pltpu.SMEM)] * scalars + [
        pl.BlockSpec(memory_space=pltpu.VMEM)
    ] * count


def scan_step(upper, arrived, through, past):
    return pl.pallas_call(
        step_kernel,
        out_shape=(
            jax.ShapeDtypeStruct(past.shape, jnp.float32),
            jax.ShapeDtypeStruct(past.shape, jnp.bfloat16),
        ),
        in_specs=in_vmem(3, 1),
        out_specs=tuple(in_vmem(2, 0)),
        cost_estimate=pl.CostEstimate(
            flops=6 * 128**3, bytes_accessed=6 * 2 * past.size, transcendentals=0
        ),
        compiler_params=pltpu.CompilerParams(vmem_limit_bytes=4 * 2**20),
        name="scan_step",
    )(upper, arrived, through, past)


def finish_kernel(upper_ref, arrived_ref, past_ref, oloc_ref, qp_ref, gain_ref, out_ref):
    upper = upper_ref[0] != 0
    other = jnp.where(upper, arrived_ref[0].astype(jnp.float32), arrived_ref[1].astype(jnp.float32))
    near = jnp.where(upper, past_ref[0], past_ref[1])
    met = composed(stacked(other), stacked(near))[HEAD_DIM:]
    kept = stacked(jnp.where(upper, past_ref[1], past_ref[0]))[HEAD_DIM:]
    ahead, behind = jnp.where(upper, met, kept), jnp.where(upper, kept, met)
    states = ahead + pltpu.roll(behind, HEAD_DIM, 1)
    summed = oloc_ref[...] + mm(states, qp_ref[...])
    center = jnp.mean(summed, axis=0, keepdims=True)
    away = summed - center
    spread = jnp.mean(away * away, axis=0, keepdims=True)
    out_ref[...] = (
        away * lax.rsqrt(spread + HEAD_DIM * 1e-05) * gain_ref[...]
    ).astype(jnp.bfloat16)


def finish_half(upper, arrived, past, oloc, qp, gain):
    return pl.pallas_call(
        finish_kernel,
        out_shape=jax.ShapeDtypeStruct(oloc.shape, jnp.bfloat16),
        in_specs=in_vmem(5, 1),
        out_specs=in_vmem(1, 0)[0],
        cost_estimate=pl.CostEstimate(
            flops=4 * 128**3 + 16 * 128**3, bytes_accessed=2**20, transcendentals=1024
        ),
        compiler_params=pltpu.CompilerParams(vmem_limit_bytes=8 * 2**20),
        name="mixer_finish",
    )(upper, arrived, past, oloc, qp, gain)


def swapped(through, distance):
    count = lax.axis_size("ep")
    return lax.ppermute(through, "ep", [(i, i ^ distance) for i in range(count)])


def side(distance):
    return (lax.axis_index("ep") & distance).reshape(1).astype(jnp.int32)


def expert_kernel(rows_ref, gate_ref, up_ref, down_ref, out_ref):
    parts = rows_ref.shape[0]
    rows = jnp.concatenate([rows_ref[j] for j in range(parts)], axis=1)
    gate = mm(rows, gate_ref[...])
    up = mm(rows, up_ref[...])
    hidden = (gate / (1.0 + jnp.exp(-gate)) * up).astype(jnp.bfloat16)
    result = mm(hidden, down_ref[...]).astype(jnp.bfloat16)
    for j in range(parts):
        out_ref[j] = result[:, j * LANES : (j + 1) * LANES]


def expert_rows(rows, gate, up, down):
    parts, total, lanes = rows.shape
    tile = 128 if total % 128 == 0 else total
    block = pl.BlockSpec((parts, tile, lanes), lambda i: (0, i, 0))
    fixed = lambda array: pl.BlockSpec(array.shape, lambda i: (0, 0))
    return pl.pallas_call(
        expert_kernel,
        grid=(total // tile,),
        in_specs=[block, fixed(gate), fixed(up), fixed(down)],
        out_specs=block,
        out_shape=jax.ShapeDtypeStruct(rows.shape, jnp.bfloat16),
        cost_estimate=pl.CostEstimate(
            flops=6 * total * gate.size,
            bytes_accessed=2 * (2 * rows.size + 3 * gate.size),
            transcendentals=total * gate.shape[1],
        ),
        compiler_params=pltpu.CompilerParams(vmem_limit_bytes=66000000),
        name="expert_rows",
    )(rows, gate, up, down)


def route_kernel(
    capacity, at_ref, rows_ref, gain_ref, routes_ref, weight_ref, outgoing_ref, combine_ref
):
    slots, total = combine_ref.shape
    full = rows_ref[...].astype(jnp.float32)
    scale = lax.rsqrt(jnp.mean(full * full, axis=1, keepdims=True) + 1e-06)
    lanes = pl.ds(pl.multiple_of(at_ref[0], LANES), LANES)
    normed = rows_ref[:, lanes].astype(jnp.float32) * scale * gain_ref[:, lanes]
    expert = lax.broadcasted_iota(jnp.int32, (LANES, total), 0)
    named = [
        jnp.where(routes_ref[k : k + 1, :] == expert, 1.0, 0.0)
        for k in range(routes_ref.shape[0])
    ]
    earlier = lax.broadcasted_iota(jnp.int32, (total, total), 0) < lax.broadcasted_iota(
        jnp.int32, (total, total), 1
    )
    before = mm(sum(named), jnp.where(earlier, 1.0, 0.0))
    slot = lax.broadcasted_iota(jnp.int32, (slots, total), 0)
    chosen = jnp.zeros((slots, total), jnp.float32)
    combine = jnp.zeros((slots, total), jnp.float32)
    for k, one in enumerate(named):
        place = jnp.sum(before * one, axis=0, keepdims=True).astype(jnp.int32)
        hit = routes_ref[k : k + 1, :] * capacity + place == slot
        chosen = jnp.where(hit, 1.0, chosen)
        combine = jnp.where(hit, weight_ref[k : k + 1, :], combine)
    outgoing_ref[...] = mm(chosen, normed).astype(jnp.bfloat16)
    combine_ref[...] = combine.astype(jnp.bfloat16)


def routed(at, rows, gain, routes, weight, slots, capacity):
    total = rows.shape[0]
    whole = lambda array: pl.BlockSpec(array.shape, lambda: (0, 0))
    return pl.pallas_call(
        functools.partial(route_kernel, capacity),
        out_shape=(
            jax.ShapeDtypeStruct((slots, LANES), jnp.bfloat16),
            jax.ShapeDtypeStruct((slots, total), jnp.bfloat16),
        ),
        in_specs=in_vmem(0, 1) + [whole(v) for v in (rows, gain, routes, weight)],
        cost_estimate=pl.CostEstimate(
            flops=4 * total * slots * LANES, bytes_accessed=2 * rows.size, transcendentals=total
        ),
        compiler_params=pltpu.CompilerParams(vmem_limit_bytes=63600000),
        name="route_rows",
    )(at, rows, gain, routes, weight)


def summed_pieces(pieces):
    return jnp.sum(pieces.astype(jnp.float32), axis=0).astype(jnp.bfloat16)


def spread(array, axis):
    return lax.all_to_all(array, axis, 0, 0, tiled=True)


def on_device(
    query_in,
    key_in,
    value_in,
    erase_pre,
    decay_pre,
    mix_gain,
    expert_in,
    expert_gain,
    routes,
    route_weight,
    gate_weight,
    up_weight,
    down_weight,
):
    experts_n, shares = lax.axis_size("ep"), lax.axis_size("tp")
    row_count, features = expert_in.shape
    capacity = 3 * routes.shape[1] * row_count // (2 * experts_n)
    slot_total = experts_n * capacity
    col_count = features // shares
    at = lax.axis_index("tp") * col_count
    outgoing, combine = routed(
        at.reshape(1).astype(jnp.int32),
        expert_in,
        expert_gain[None],
        routes.T,
        route_weight.T,
        slot_total,
        capacity,
    )
    arrived = spread(outgoing.reshape(experts_n, capacity, col_count), "ep").reshape(
        slot_total, col_count
    )
    middle = slot_total // 2
    copies = [
        jnp.broadcast_to(part[None], (shares, *part.shape))
        for part in (arrived[:middle], arrived[middle:])
    ]
    copies[0], query_in = lax.optimization_barrier((copies[0], query_in))
    shared_a = spread(copies[0], "tp")
    oloc, qp, own_maps = local_half(query_in, key_in, value_in, erase_pre, decay_pre)
    past, through = jnp.zeros(own_maps.shape, jnp.float32), own_maps
    weights = [gate_weight[0], up_weight[0], down_weight[0]]
    shared_a, copies[1], past, through = lax.optimization_barrier(
        (shared_a, copies[1], past, through)
    )

    def scanned(steps, past, through):
        for step in steps:
            past, through = scan_step(side(step), swapped(through, step), through, past)
        return past, through

    shared_b = spread(copies[1], "tp")
    partial_a = expert_rows(shared_a, *weights)
    past, through = scanned((1, 2), past, through)
    shared_b, partial_a, past, through = lax.optimization_barrier(
        (shared_b, partial_a, past, through)
    )
    pieces_a = spread(partial_a, "tp")
    partial_b = expert_rows(shared_b, *weights)
    past, through = scanned((4,), past, through)
    pieces_a, partial_b, past, through = lax.optimization_barrier(
        (pieces_a, partial_b, past, through)
    )
    pieces_b = spread(partial_b, "tp")
    summed_a = summed_pieces(pieces_a)
    past, through = scanned((8,), past, through)
    pieces_b, summed_a, past, through = lax.optimization_barrier(
        (pieces_b, summed_a, past, through)
    )
    summed = jnp.concatenate([summed_a, summed_pieces(pieces_b)], axis=0)
    returned = spread(summed.reshape(experts_n, capacity, col_count), "ep").reshape(
        slot_total, col_count
    )
    distance = experts_n // 2
    crossing = swapped(through, distance)
    mixer_out = finish_half(side(distance), crossing, past, oloc, qp, mix_gain[:, None])
    expert_out = mm_tn(combine, returned).astype(jnp.bfloat16)
    return (mixer_out, expert_out)


def solution(mesh):
    placed = (
        P("tp", "ep"),
        P("tp", "ep"),
        P("tp", "ep"),
        P("tp", "ep"),
        P("tp", "ep"),
        P("tp"),
        P("ep", None),
        P(),
        P("ep", None),
        P("ep", None),
        P("ep", None, "tp"),
        P("ep", None, "tp"),
        P("ep", "tp", None),
    )
    return jax.shard_map(
        on_device,
        mesh=mesh,
        in_specs=placed,
        out_specs=(P("tp", "ep"), P("ep", "tp")),
        check_vma=False,
    )
```

```python
import functools

import jax
import jax.numpy as jnp
from jax import lax
from jax.experimental import pallas as pl
from jax.experimental.pallas import tpu as pltpu
from jax.sharding import PartitionSpec as P

HEAD_DIM = 64
LANES = 128
SPAN = 128
UNROLL = 2
DECAY_SCALE = 0.6065306597126334


def mm(a, b):
    return jnp.dot(
        a.astype(jnp.bfloat16), b.astype(jnp.bfloat16), preferred_element_type=jnp.float32
    )


def mm_tn(a, b):
    return lax.dot_general(
        a.astype(jnp.bfloat16),
        b.astype(jnp.bfloat16),
        (((0,), (0,)), ((), ())),
        preferred_element_type=jnp.float32,
    )


def mm_nt(a, b):
    return lax.dot_general(
        a.astype(jnp.bfloat16),
        b.astype(jnp.bfloat16),
        (((1,), (1,)), ((), ())),
        preferred_element_type=jnp.float32,
    )


def local_kernel(
    q_ref, k_ref, v_ref, e_ref, d_ref, oloc_ref, qp_ref, maps_ref,
    uk_ref, er_ref, lk_ref, qh_f_ref, qh_b_ref, z_ref, b_ref, dec_ref,
):
    count = q_ref.shape[1] // SPAN
    kf = k_ref[...].astype(jnp.float32)
    uk = kf * lax.rsqrt(jnp.sum(kf * kf, axis=0, keepdims=True) + 1e-05)
    uk_ref[...] = uk
    er_ref[...] = uk * (1.0 / (1.0 + jnp.exp(-e_ref[...].astype(jnp.float32))))
    lk_ref[...] = -DECAY_SCALE / (1.0 + jnp.exp(-d_ref[...].astype(jnp.float32)))

    row = lax.broadcasted_iota(jnp.int32, (SPAN, SPAN), 0)
    col = lax.broadcasted_iota(jnp.int32, (SPAN, SPAN), 1)
    differ = row ^ col
    eye_span = jnp.where(differ == 0, 1.0, 0.0)
    running = jnp.where(row <= col, 1.0, 0.0).astype(jnp.bfloat16)
    eye = jnp.where(
        lax.broadcasted_iota(jnp.int32, (HEAD_DIM, HEAD_DIM), 0)
        == lax.broadcasted_iota(jnp.int32, (HEAD_DIM, HEAD_DIM), 1),
        1.0,
        0.0,
    )
    strict = (row < col, row > col)
    inclusive = (row <= col, row >= col)

    def body(step, carry):
        units = []
        for part in range(UNROLL):
            chunk = step * UNROLL + part
            lanes = pl.ds(pl.multiple_of(chunk * SPAN, SPAN), SPAN)
            q = q_ref[:, lanes].astype(jnp.float32)
            k = k_ref[:, lanes].astype(jnp.float32)
            v = v_ref[:, lanes]
            u, er, lk = uk_ref[:, lanes], er_ref[:, lanes], lk_ref[:, lanes]
            high = lk.astype(jnp.bfloat16)
            rest = lk - high.astype(jnp.float32)
            low = rest.astype(jnp.bfloat16)
            sums = mm(jnp.concatenate([high, low], axis=0), running)
            cum = sums[:HEAD_DIM] + sums[HEAD_DIM:]
            prior = cum - lk
            last = cum[:, SPAN - 1 :]
            to_prior, fade = jnp.exp(prior), jnp.exp(last - cum)
            up_f, up_b = jnp.exp(-cum), jnp.exp(prior - last)
            dec_ref[chunk] = jnp.sum(eye * jnp.exp(last), axis=0, keepdims=True)
            both = (
                (u * to_prior, q * jnp.exp(cum), k * up_f, er * up_f, k * fade, er * fade),
                (u * fade, q * jnp.exp(last - prior), k * up_b, er * up_b, k * to_prior, er * to_prior),
            )
            for way in (0, 1):
                units.append((chunk, lanes, way, v, both[way]))
        state = []
        for chunk, lanes, way, v, (ud, qd, ku, eu, kend, eend) in units:
            gram = mm_tn(
                jnp.concatenate([ku, eu], axis=1), jnp.concatenate([ud, qd], axis=1)
            )
            k_mix = jnp.where(strict[way], gram[:SPAN, :SPAN], 0.0).astype(jnp.bfloat16)
            k_read = jnp.where(inclusive[way], gram[:SPAN, SPAN:], 0.0).astype(jnp.bfloat16)
            e_mix = jnp.where(strict[way], gram[SPAN:, :SPAN], 0.0)
            e_read = jnp.where(inclusive[way], gram[SPAN:, SPAN:], 0.0).astype(jnp.bfloat16)
            inv = (eye_span - jnp.where(differ == 1, e_mix, 0.0)).astype(jnp.bfloat16)
            mixed = mm(v, jnp.concatenate([k_mix, k_read], axis=1))
            state.append([e_mix, inv, mixed, e_read])
        width = 2
        while width < SPAN:
            inside = (differ >= width) & (differ < 2 * width)
            halves = [mm(inv, jnp.where(inside, e_mix, 0.0)) for e_mix, inv, _, _ in state]
            for unit, half in zip(state, halves):
                unit[1] = (unit[1].astype(jnp.float32) - mm(half, unit[1])).astype(jnp.bfloat16)
            width *= 2
        for (chunk, lanes, way, v, (ud, qd, ku, eu, kend, eend)), (_, inv, mixed, e_read) in zip(
            units, state
        ):
            solved = mm(jnp.concatenate([ud, mixed[:, :SPAN]], axis=0), inv).astype(jnp.bfloat16)
            read = mm(solved, e_read)
            ends = mm_nt(solved, eend)
            qh = (qh_f_ref, qh_b_ref)[way]
            qh[:, lanes] = (qd - read[:HEAD_DIM]).astype(jnp.bfloat16)
            out = mixed[:, SPAN:] - read[HEAD_DIM:]
            if way == 0:
                oloc_ref[:, lanes] = out
            else:
                oloc_ref[:, lanes] += out
            z_ref[way, chunk] = ends[:HEAD_DIM].astype(jnp.bfloat16)
            b_ref[way, chunk] = mm_nt(v, kend) - ends[HEAD_DIM:]
        return carry

    lax.fori_loop(0, count // UNROLL, body, 0)

    start = jnp.concatenate([jnp.zeros_like(eye), eye], axis=0)
    carried = [start, start]
    for step in range(count):
        for way, qh in ((0, qh_f_ref), (1, qh_b_ref)):
            chunk = step if way == 0 else count - 1 - step
            lanes = slice(chunk * SPAN, (chunk + 1) * SPAN)
            now = carried[way]
            narrow = now.astype(jnp.bfloat16)
            read = mm(narrow, qh[:, lanes])
            oloc_ref[:, lanes] += read[:HEAD_DIM]
            qp_ref[way * HEAD_DIM : (way + 1) * HEAD_DIM, lanes] = read[HEAD_DIM:].astype(jnp.bfloat16)
            moved = now * dec_ref[chunk] - mm(narrow, z_ref[way, chunk])
            carried[way] = jnp.concatenate(
                [moved[:HEAD_DIM] + b_ref[way, chunk], moved[HEAD_DIM:]], axis=0
            )
    for way in (0, 1):
        maps_ref[way] = jnp.concatenate(
            [carried[way][:HEAD_DIM], carried[way][HEAD_DIM:] - eye], axis=1
        ).astype(jnp.bfloat16)


def local_half(query, key, value, erase, decay):
    tokens = query.shape[1]
    count = tokens // SPAN
    full = lambda kind: jax.ShapeDtypeStruct((HEAD_DIM, tokens), kind)
    whole = lambda kind: pltpu.VMEM((HEAD_DIM, tokens), kind)
    return pl.pallas_call(
        local_kernel,
        out_shape=(
            full(jnp.float32),
            jax.ShapeDtypeStruct((2 * HEAD_DIM, tokens), jnp.bfloat16),
            jax.ShapeDtypeStruct((2, HEAD_DIM, 2 * HEAD_DIM), jnp.bfloat16),
        ),
        scratch_shapes=[
            whole(jnp.float32),
            whole(jnp.float32),
            whole(jnp.float32),
            whole(jnp.bfloat16),
            whole(jnp.bfloat16),
            pltpu.VMEM((2, count, HEAD_DIM, HEAD_DIM), jnp.bfloat16),
            pltpu.VMEM((2, count, HEAD_DIM, HEAD_DIM), jnp.float32),
            pltpu.VMEM((count, 1, HEAD_DIM), jnp.float32),
        ],
        cost_estimate=pl.CostEstimate(
            flops=16 * 22 * 2 * 128**3, bytes_accessed=tokens * 64 * 18, transcendentals=tokens * 64 * 9
        ),
        compiler_params=pltpu.CompilerParams(vmem_limit_bytes=66000000),
        name="mixer_local",
    )(query, key, value, erase, decay)


def stacked(wide):
    left = lax.broadcasted_iota(jnp.int32, (2 * HEAD_DIM, 2 * HEAD_DIM), 1) < HEAD_DIM
    full = wide.astype(jnp.float32)
    return jnp.where(left, jnp.concatenate([pltpu.roll(full, HEAD_DIM, 1), full], axis=0), 0.0)


def widened(tall):
    return tall[HEAD_DIM:] + pltpu.roll(tall[:HEAD_DIM], HEAD_DIM, 1)


def composed(first, later):
    return first + mm(first, later) + later


def step_kernel(upper_ref, arrived_ref, through_ref, past_ref, next_past_ref, next_through_ref):
    upper = upper_ref[0] != 0
    other = [stacked(arrived_ref[way]) for way in (0, 1)]
    mine = [stacked(through_ref[way]) for way in (0, 1)]
    near = jnp.where(upper, past_ref[0], past_ref[1])
    met = widened(composed(jnp.where(upper, other[0], other[1]), stacked(near)))
    next_past_ref[0] = jnp.where(upper, met, past_ref[0])
    next_past_ref[1] = jnp.where(upper, past_ref[1], met)
    for way in (0, 1):
        other_first = upper if way == 0 else jnp.logical_not(upper)
        first = jnp.where(other_first, other[way], mine[way])
        later = jnp.where(other_first, mine[way], other[way])
        next_through_ref[way] = widened(composed(first, later)).astype(jnp.bfloat16)


def in_vmem(count, scalars):
    return [pl.BlockSpec(memory_space=pltpu.SMEM)] * scalars + [
        pl.BlockSpec(memory_space=pltpu.VMEM)
    ] * count


def scan_step(upper, arrived, through, past):
    return pl.pallas_call(
        step_kernel,
        out_shape=(
            jax.ShapeDtypeStruct(past.shape, jnp.float32),
            jax.ShapeDtypeStruct(past.shape, jnp.bfloat16),
        ),
        in_specs=in_vmem(3, 1),
        out_specs=tuple(in_vmem(2, 0)),
        cost_estimate=pl.CostEstimate(
            flops=6 * 128**3, bytes_accessed=6 * 2 * past.size, transcendentals=0
        ),
        compiler_params=pltpu.CompilerParams(vmem_limit_bytes=66000000),
        name="scan_step",
    )(upper, arrived, through, past)


def finish_kernel(upper_ref, arrived_ref, past_ref, oloc_ref, qp_ref, gain_ref, out_ref):
    upper = upper_ref[0] != 0
    other = jnp.where(upper, arrived_ref[0].astype(jnp.float32), arrived_ref[1].astype(jnp.float32))
    near = jnp.where(upper, past_ref[0], past_ref[1])
    met = composed(stacked(other), stacked(near))[HEAD_DIM:]
    kept = stacked(jnp.where(upper, past_ref[1], past_ref[0]))[HEAD_DIM:]
    ahead, behind = jnp.where(upper, met, kept), jnp.where(upper, kept, met)
    states = ahead + pltpu.roll(behind, HEAD_DIM, 1)
    summed = oloc_ref[...] + mm(states, qp_ref[...])
    center = jnp.mean(summed, axis=0, keepdims=True)
    away = summed - center
    spread = jnp.mean(away * away, axis=0, keepdims=True)
    out_ref[...] = (
        away * lax.rsqrt(spread + HEAD_DIM * 1e-05) * gain_ref[...]
    ).astype(jnp.bfloat16)


def finish_half(upper, arrived, past, oloc, qp, gain):
    return pl.pallas_call(
        finish_kernel,
        out_shape=jax.ShapeDtypeStruct(oloc.shape, jnp.bfloat16),
        in_specs=in_vmem(5, 1),
        out_specs=in_vmem(1, 0)[0],
        cost_estimate=pl.CostEstimate(
            flops=4 * 128**3 + 16 * 128**3, bytes_accessed=2**20, transcendentals=1024
        ),
        compiler_params=pltpu.CompilerParams(vmem_limit_bytes=8 * 2**20),
        name="mixer_finish",
    )(upper, arrived, past, oloc, qp, gain)


def swapped(through, distance):
    count = lax.axis_size("ep")
    return lax.ppermute(through, "ep", [(i, i ^ distance) for i in range(count)])


def side(distance):
    return (lax.axis_index("ep") & distance).reshape(1).astype(jnp.int32)


def expert_kernel(rows_ref, gate_ref, up_ref, down_ref, out_ref):
    parts = rows_ref.shape[0]
    rows = jnp.concatenate([rows_ref[j] for j in range(parts)], axis=1)
    gate = mm(rows, gate_ref[...])
    up = mm(rows, up_ref[...])
    hidden = (gate / (1.0 + jnp.exp(-gate)) * up).astype(jnp.bfloat16)
    result = mm(hidden, down_ref[...]).astype(jnp.bfloat16)
    for j in range(parts):
        out_ref[j] = result[:, j * LANES : (j + 1) * LANES]


def expert_rows(rows, gate, up, down):
    parts, total, lanes = rows.shape
    tile = 128 if total % 128 == 0 else total
    block = pl.BlockSpec((parts, tile, lanes), lambda i: (0, i, 0))
    fixed = lambda array: pl.BlockSpec(array.shape, lambda i: (0, 0))
    return pl.pallas_call(
        expert_kernel,
        grid=(total // tile,),
        in_specs=[block, fixed(gate), fixed(up), fixed(down)],
        out_specs=block,
        out_shape=jax.ShapeDtypeStruct(rows.shape, jnp.bfloat16),
        cost_estimate=pl.CostEstimate(
            flops=6 * total * gate.size,
            bytes_accessed=2 * (2 * rows.size + 3 * gate.size),
            transcendentals=total * gate.shape[1],
        ),
        compiler_params=pltpu.CompilerParams(vmem_limit_bytes=66000000),
        name="expert_rows",
    )(rows, gate, up, down)


def route_kernel(
    capacity, at_ref, rows_ref, gain_ref, routes_ref, weight_ref, outgoing_ref, combine_ref
):
    slots, total = combine_ref.shape
    full = rows_ref[...].astype(jnp.float32)
    scale = lax.rsqrt(jnp.mean(full * full, axis=1, keepdims=True) + 1e-06)
    lanes = pl.ds(pl.multiple_of(at_ref[0], LANES), LANES)
    normed = rows_ref[:, lanes].astype(jnp.float32) * scale * gain_ref[:, lanes]
    expert = lax.broadcasted_iota(jnp.int32, (LANES, total), 0)
    named = [
        jnp.where(routes_ref[k : k + 1, :] == expert, 1.0, 0.0)
        for k in range(routes_ref.shape[0])
    ]
    earlier = lax.broadcasted_iota(jnp.int32, (total, total), 0) < lax.broadcasted_iota(
        jnp.int32, (total, total), 1
    )
    before = mm(sum(named), jnp.where(earlier, 1.0, 0.0))
    slot = lax.broadcasted_iota(jnp.int32, (slots, total), 0)
    chosen = jnp.zeros((slots, total), jnp.float32)
    combine = jnp.zeros((slots, total), jnp.float32)
    for k, one in enumerate(named):
        place = jnp.sum(before * one, axis=0, keepdims=True).astype(jnp.int32)
        hit = routes_ref[k : k + 1, :] * capacity + place == slot
        chosen = jnp.where(hit, 1.0, chosen)
        combine = jnp.where(hit, weight_ref[k : k + 1, :], combine)
    outgoing_ref[...] = mm(chosen, normed).astype(jnp.bfloat16)
    combine_ref[...] = combine.astype(jnp.bfloat16)


def routed(at, rows, gain, routes, weight, slots, capacity):
    total = rows.shape[0]
    whole = lambda array: pl.BlockSpec(array.shape, lambda: (0, 0))
    return pl.pallas_call(
        functools.partial(route_kernel, capacity),
        out_shape=(
            jax.ShapeDtypeStruct((slots, LANES), jnp.bfloat16),
            jax.ShapeDtypeStruct((slots, total), jnp.bfloat16),
        ),
        in_specs=in_vmem(0, 1) + [whole(v) for v in (rows, gain, routes, weight)],
        cost_estimate=pl.CostEstimate(
            flops=4 * total * slots * LANES, bytes_accessed=2 * rows.size, transcendentals=total
        ),
        compiler_params=pltpu.CompilerParams(vmem_limit_bytes=63600000),
        name="route_rows",
    )(at, rows, gain, routes, weight)


def summed_pieces(pieces):
    return jnp.sum(pieces.astype(jnp.float32), axis=0).astype(jnp.bfloat16)


def spread(array, axis):
    return lax.all_to_all(array, axis, 0, 0, tiled=True)


def on_device(
    query_in,
    key_in,
    value_in,
    erase_pre,
    decay_pre,
    mix_gain,
    expert_in,
    expert_gain,
    routes,
    route_weight,
    gate_weight,
    up_weight,
    down_weight,
):
    experts_n, shares = lax.axis_size("ep"), lax.axis_size("tp")
    row_count, features = expert_in.shape
    capacity = 3 * routes.shape[1] * row_count // (2 * experts_n)
    slot_total = experts_n * capacity
    col_count = features // shares
    at = lax.axis_index("tp") * col_count
    outgoing, combine = routed(
        at.reshape(1).astype(jnp.int32),
        expert_in,
        expert_gain[None],
        routes.T,
        route_weight.T,
        slot_total,
        capacity,
    )
    arrived = spread(outgoing.reshape(experts_n, capacity, col_count), "ep").reshape(
        slot_total, col_count
    )
    oloc, qp, own_maps = local_half(query_in, key_in, value_in, erase_pre, decay_pre)
    arrived, own_maps = lax.optimization_barrier((arrived, own_maps))
    middle = slot_total // 2
    copies = [
        jnp.broadcast_to(part[None], (shares, *part.shape))
        for part in (arrived[:middle], arrived[middle:])
    ]
    copies[0], own_maps = lax.optimization_barrier((copies[0], own_maps))
    shared_a = spread(copies[0], "tp")
    past, through = jnp.zeros(own_maps.shape, jnp.float32), own_maps
    weights = [gate_weight[0], up_weight[0], down_weight[0]]

    def scanned(steps, past, through):
        for step in steps:
            past, through = scan_step(side(step), swapped(through, step), through, past)
        return past, through

    past, through = scanned((1,), past, through)
    copies[1], past, through = lax.optimization_barrier((copies[1], past, through))
    past, through = scanned((2,), past, through)
    shared_a, copies[1], past, through = lax.optimization_barrier(
        (shared_a, copies[1], past, through)
    )
    shared_b = spread(copies[1], "tp")
    partial_a = expert_rows(shared_a, *weights)
    past, through = scanned((4,), past, through)
    shared_b, partial_a, past, through = lax.optimization_barrier(
        (shared_b, partial_a, past, through)
    )
    pieces_a = spread(partial_a, "tp")
    partial_b = expert_rows(shared_b, *weights)
    past, through = scanned((8,), past, through)
    pieces_a, partial_b, past, through = lax.optimization_barrier(
        (pieces_a, partial_b, past, through)
    )
    pieces_b = spread(partial_b, "tp")
    summed_a = summed_pieces(pieces_a)
    distance = experts_n // 2
    crossing = swapped(through, distance)
    pieces_b, summed_a, crossing = lax.optimization_barrier((pieces_b, summed_a, crossing))
    summed = jnp.concatenate([summed_a, summed_pieces(pieces_b)], axis=0)
    returned = spread(summed.reshape(experts_n, capacity, col_count), "ep").reshape(
        slot_total, col_count
    )
    mixer_out = finish_half(side(distance), crossing, past, oloc, qp, mix_gain[:, None])
    expert_out = mm_tn(combine, returned).astype(jnp.bfloat16)
    return (mixer_out, expert_out)


def solution(mesh):
    placed = (
        P("tp", "ep"),
        P("tp", "ep"),
        P("tp", "ep"),
        P("tp", "ep"),
        P("tp", "ep"),
        P("tp"),
        P("ep", None),
        P(),
        P("ep", None),
        P("ep", None),
        P("ep", None, "tp"),
        P("ep", None, "tp"),
        P("ep", "tp", None),
    )
    return jax.shard_map(
        on_device,
        mesh=mesh,
        in_specs=placed,
        out_specs=(P("tp", "ep"), P("ep", "tp")),
        check_vma=False,
    )
```

```python
import functools

import jax
import jax.numpy as jnp
from jax import lax
from jax.experimental import pallas as pl
from jax.experimental.pallas import tpu as pltpu
from jax.sharding import PartitionSpec as P

HEAD_DIM = 64
LANES = 128
SPAN = 128
UNROLL = 2
DECAY_SCALE = 0.6065306597126334


def mm(a, b):
    return jnp.dot(
        a.astype(jnp.bfloat16), b.astype(jnp.bfloat16), preferred_element_type=jnp.float32
    )


def mm_tn(a, b):
    return lax.dot_general(
        a.astype(jnp.bfloat16),
        b.astype(jnp.bfloat16),
        (((0,), (0,)), ((), ())),
        preferred_element_type=jnp.float32,
    )


def mm_nt(a, b):
    return lax.dot_general(
        a.astype(jnp.bfloat16),
        b.astype(jnp.bfloat16),
        (((1,), (1,)), ((), ())),
        preferred_element_type=jnp.float32,
    )


def local_kernel(
    q_ref, k_ref, v_ref, e_ref, d_ref, oloc_ref, qp_ref, maps_ref,
    uk_ref, er_ref, lk_ref, qh_f_ref, qh_b_ref, z_ref, b_ref, dec_ref,
):
    count = q_ref.shape[1] // SPAN
    kf = k_ref[...].astype(jnp.float32)
    uk = kf * lax.rsqrt(jnp.sum(kf * kf, axis=0, keepdims=True) + 1e-05)
    uk_ref[...] = uk
    er_ref[...] = uk * (1.0 / (1.0 + jnp.exp(-e_ref[...].astype(jnp.float32))))
    lk_ref[...] = -DECAY_SCALE / (1.0 + jnp.exp(-d_ref[...].astype(jnp.float32)))

    row = lax.broadcasted_iota(jnp.int32, (SPAN, SPAN), 0)
    col = lax.broadcasted_iota(jnp.int32, (SPAN, SPAN), 1)
    differ = row ^ col
    eye_span = jnp.where(differ == 0, 1.0, 0.0)
    running = jnp.where(row <= col, 1.0, 0.0).astype(jnp.bfloat16)
    eye = jnp.where(
        lax.broadcasted_iota(jnp.int32, (HEAD_DIM, HEAD_DIM), 0)
        == lax.broadcasted_iota(jnp.int32, (HEAD_DIM, HEAD_DIM), 1),
        1.0,
        0.0,
    )
    strict = (row < col, row > col)
    inclusive = (row <= col, row >= col)

    def body(step, carry):
        units = []
        for part in range(UNROLL):
            chunk = step * UNROLL + part
            lanes = pl.ds(pl.multiple_of(chunk * SPAN, SPAN), SPAN)
            q = q_ref[:, lanes].astype(jnp.float32)
            k = k_ref[:, lanes].astype(jnp.float32)
            v = v_ref[:, lanes]
            u, er, lk = uk_ref[:, lanes], er_ref[:, lanes], lk_ref[:, lanes]
            high = lk.astype(jnp.bfloat16)
            rest = lk - high.astype(jnp.float32)
            low = rest.astype(jnp.bfloat16)
            sums = mm(jnp.concatenate([high, low], axis=0), running)
            cum = sums[:HEAD_DIM] + sums[HEAD_DIM:]
            prior = cum - lk
            last = cum[:, SPAN - 1 :]
            to_prior, fade = jnp.exp(prior), jnp.exp(last - cum)
            up_f, up_b = jnp.exp(-cum), jnp.exp(prior - last)
            dec_ref[chunk] = jnp.sum(eye * jnp.exp(last), axis=0, keepdims=True)
            both = (
                (u * to_prior, q * jnp.exp(cum), k * up_f, er * up_f, k * fade, er * fade),
                (u * fade, q * jnp.exp(last - prior), k * up_b, er * up_b, k * to_prior, er * to_prior),
            )
            for way in (0, 1):
                units.append((chunk, lanes, way, v, both[way]))
        state = []
        for chunk, lanes, way, v, (ud, qd, ku, eu, kend, eend) in units:
            gram = mm_tn(
                jnp.concatenate([ku, eu], axis=1), jnp.concatenate([ud, qd], axis=1)
            )
            k_mix = jnp.where(strict[way], gram[:SPAN, :SPAN], 0.0).astype(jnp.bfloat16)
            k_read = jnp.where(inclusive[way], gram[:SPAN, SPAN:], 0.0).astype(jnp.bfloat16)
            e_mix = jnp.where(strict[way], gram[SPAN:, :SPAN], 0.0)
            e_read = jnp.where(inclusive[way], gram[SPAN:, SPAN:], 0.0).astype(jnp.bfloat16)
            inv = (eye_span - jnp.where(differ == 1, e_mix, 0.0)).astype(jnp.bfloat16)
            mixed = mm(v, jnp.concatenate([k_mix, k_read], axis=1))
            state.append([e_mix, inv, mixed, e_read])
        width = 2
        while width < SPAN:
            inside = (differ >= width) & (differ < 2 * width)
            halves = [mm(inv, jnp.where(inside, e_mix, 0.0)) for e_mix, inv, _, _ in state]
            for unit, half in zip(state, halves):
                unit[1] = (unit[1].astype(jnp.float32) - mm(half, unit[1])).astype(jnp.bfloat16)
            width *= 2
        for (chunk, lanes, way, v, (ud, qd, ku, eu, kend, eend)), (_, inv, mixed, e_read) in zip(
            units, state
        ):
            solved = mm(jnp.concatenate([ud, mixed[:, :SPAN]], axis=0), inv).astype(jnp.bfloat16)
            read = mm(solved, e_read)
            ends = mm_nt(solved, eend)
            qh = (qh_f_ref, qh_b_ref)[way]
            qh[:, lanes] = (qd - read[:HEAD_DIM]).astype(jnp.bfloat16)
            out = mixed[:, SPAN:] - read[HEAD_DIM:]
            if way == 0:
                oloc_ref[:, lanes] = out
            else:
                oloc_ref[:, lanes] += out
            z_ref[way, chunk] = ends[:HEAD_DIM].astype(jnp.bfloat16)
            b_ref[way, chunk] = mm_nt(v, kend) - ends[HEAD_DIM:]
        return carry

    lax.fori_loop(0, count // UNROLL, body, 0)

    start = jnp.concatenate([jnp.zeros_like(eye), eye], axis=0)
    carried = [start, start]
    for step in range(count):
        for way, qh in ((0, qh_f_ref), (1, qh_b_ref)):
            chunk = step if way == 0 else count - 1 - step
            lanes = slice(chunk * SPAN, (chunk + 1) * SPAN)
            now = carried[way]
            narrow = now.astype(jnp.bfloat16)
            read = mm(narrow, qh[:, lanes])
            oloc_ref[:, lanes] += read[:HEAD_DIM]
            qp_ref[way * HEAD_DIM : (way + 1) * HEAD_DIM, lanes] = read[HEAD_DIM:].astype(jnp.bfloat16)
            moved = now * dec_ref[chunk] - mm(narrow, z_ref[way, chunk])
            carried[way] = jnp.concatenate(
                [moved[:HEAD_DIM] + b_ref[way, chunk], moved[HEAD_DIM:]], axis=0
            )
    for way in (0, 1):
        maps_ref[way] = jnp.concatenate(
            [carried[way][:HEAD_DIM], carried[way][HEAD_DIM:] - eye], axis=1
        ).astype(jnp.bfloat16)


def local_half(query, key, value, erase, decay):
    tokens = query.shape[1]
    count = tokens // SPAN
    full = lambda kind: jax.ShapeDtypeStruct((HEAD_DIM, tokens), kind)
    whole = lambda kind: pltpu.VMEM((HEAD_DIM, tokens), kind)
    return pl.pallas_call(
        local_kernel,
        out_shape=(
            full(jnp.float32),
            jax.ShapeDtypeStruct((2 * HEAD_DIM, tokens), jnp.bfloat16),
            jax.ShapeDtypeStruct((2, HEAD_DIM, 2 * HEAD_DIM), jnp.bfloat16),
        ),
        scratch_shapes=[
            whole(jnp.float32),
            whole(jnp.float32),
            whole(jnp.float32),
            whole(jnp.bfloat16),
            whole(jnp.bfloat16),
            pltpu.VMEM((2, count, HEAD_DIM, HEAD_DIM), jnp.bfloat16),
            pltpu.VMEM((2, count, HEAD_DIM, HEAD_DIM), jnp.float32),
            pltpu.VMEM((count, 1, HEAD_DIM), jnp.float32),
        ],
        cost_estimate=pl.CostEstimate(
            flops=16 * 22 * 2 * 128**3, bytes_accessed=tokens * 64 * 18, transcendentals=tokens * 64 * 9
        ),
        compiler_params=pltpu.CompilerParams(vmem_limit_bytes=66000000),
        name="mixer_local",
    )(query, key, value, erase, decay)


def stacked(wide):
    left = lax.broadcasted_iota(jnp.int32, (2 * HEAD_DIM, 2 * HEAD_DIM), 1) < HEAD_DIM
    full = wide.astype(jnp.float32)
    return jnp.where(left, jnp.concatenate([pltpu.roll(full, HEAD_DIM, 1), full], axis=0), 0.0)


def widened(tall):
    return tall[HEAD_DIM:] + pltpu.roll(tall[:HEAD_DIM], HEAD_DIM, 1)


def composed(first, later):
    return first + mm(first, later) + later


def step_kernel(upper_ref, arrived_ref, through_ref, past_ref, next_past_ref, next_through_ref):
    upper = upper_ref[0] != 0
    other = [stacked(arrived_ref[way]) for way in (0, 1)]
    mine = [stacked(through_ref[way]) for way in (0, 1)]
    near = jnp.where(upper, past_ref[0], past_ref[1])
    met = widened(composed(jnp.where(upper, other[0], other[1]), stacked(near)))
    next_past_ref[0] = jnp.where(upper, met, past_ref[0])
    next_past_ref[1] = jnp.where(upper, past_ref[1], met)
    for way in (0, 1):
        other_first = upper if way == 0 else jnp.logical_not(upper)
        first = jnp.where(other_first, other[way], mine[way])
        later = jnp.where(other_first, mine[way], other[way])
        next_through_ref[way] = widened(composed(first, later)).astype(jnp.bfloat16)


def in_vmem(count, scalars):
    return [pl.BlockSpec(memory_space=pltpu.SMEM)] * scalars + [
        pl.BlockSpec(memory_space=pltpu.VMEM)
    ] * count


def scan_step(upper, arrived, through, past):
    return pl.pallas_call(
        step_kernel,
        out_shape=(
            jax.ShapeDtypeStruct(past.shape, jnp.float32),
            jax.ShapeDtypeStruct(past.shape, jnp.bfloat16),
        ),
        in_specs=in_vmem(3, 1),
        out_specs=tuple(in_vmem(2, 0)),
        cost_estimate=pl.CostEstimate(
            flops=6 * 128**3, bytes_accessed=6 * 2 * past.size, transcendentals=0
        ),
        compiler_params=pltpu.CompilerParams(vmem_limit_bytes=66000000),
        name="scan_step",
    )(upper, arrived, through, past)


def finish_kernel(upper_ref, arrived_ref, past_ref, oloc_ref, qp_ref, gain_ref, out_ref):
    upper = upper_ref[0] != 0
    other = jnp.where(upper, arrived_ref[0].astype(jnp.float32), arrived_ref[1].astype(jnp.float32))
    near = jnp.where(upper, past_ref[0], past_ref[1])
    met = composed(stacked(other), stacked(near))[HEAD_DIM:]
    kept = stacked(jnp.where(upper, past_ref[1], past_ref[0]))[HEAD_DIM:]
    ahead, behind = jnp.where(upper, met, kept), jnp.where(upper, kept, met)
    states = ahead + pltpu.roll(behind, HEAD_DIM, 1)
    summed = oloc_ref[...] + mm(states, qp_ref[...])
    center = jnp.mean(summed, axis=0, keepdims=True)
    away = summed - center
    spread = jnp.mean(away * away, axis=0, keepdims=True)
    out_ref[...] = (
        away * lax.rsqrt(spread + HEAD_DIM * 1e-05) * gain_ref[...]
    ).astype(jnp.bfloat16)


def finish_half(upper, arrived, past, oloc, qp, gain):
    return pl.pallas_call(
        finish_kernel,
        out_shape=jax.ShapeDtypeStruct(oloc.shape, jnp.bfloat16),
        in_specs=in_vmem(5, 1),
        out_specs=in_vmem(1, 0)[0],
        cost_estimate=pl.CostEstimate(
            flops=4 * 128**3 + 16 * 128**3, bytes_accessed=2**20, transcendentals=1024
        ),
        compiler_params=pltpu.CompilerParams(vmem_limit_bytes=8 * 2**20),
        name="mixer_finish",
    )(upper, arrived, past, oloc, qp, gain)


def swapped(through, distance):
    count = lax.axis_size("ep")
    return lax.ppermute(through, "ep", [(i, i ^ distance) for i in range(count)])


def side(distance):
    return (lax.axis_index("ep") & distance).reshape(1).astype(jnp.int32)


def expert_kernel(rows_ref, gate_ref, up_ref, down_ref, out_ref):
    parts = rows_ref.shape[0]
    rows = jnp.concatenate([rows_ref[j] for j in range(parts)], axis=1)
    gate = mm_nt(rows, gate_ref[...])
    up = mm_nt(rows, up_ref[...])
    hidden = (gate / (1.0 + jnp.exp(-gate)) * up).astype(jnp.bfloat16)
    result = mm(hidden, down_ref[...]).astype(jnp.bfloat16)
    for j in range(parts):
        out_ref[j] = result[:, j * LANES : (j + 1) * LANES]


def expert_rows(rows, gate, up, down):
    parts, total, lanes = rows.shape
    tile = 128 if total % 128 == 0 else total
    block = pl.BlockSpec((parts, tile, lanes), lambda i: (0, i, 0))
    fixed = lambda array: pl.BlockSpec(array.shape, lambda i: (0, 0))
    return pl.pallas_call(
        expert_kernel,
        grid=(total // tile,),
        in_specs=[block, fixed(gate), fixed(up), fixed(down)],
        out_specs=block,
        out_shape=jax.ShapeDtypeStruct(rows.shape, jnp.bfloat16),
        cost_estimate=pl.CostEstimate(
            flops=6 * total * gate.size,
            bytes_accessed=2 * (2 * rows.size + 3 * gate.size),
            transcendentals=total * gate.shape[0],
        ),
        compiler_params=pltpu.CompilerParams(vmem_limit_bytes=66000000),
        name="expert_rows",
    )(rows, gate, up, down)


def route_kernel(
    capacity, at_ref, rows_ref, gain_ref, routes_ref, weight_ref, outgoing_ref, combine_ref
):
    slots, total = combine_ref.shape
    full = rows_ref[...].astype(jnp.float32)
    scale = lax.rsqrt(jnp.mean(full * full, axis=1, keepdims=True) + 1e-06)
    lanes = pl.ds(pl.multiple_of(at_ref[0], LANES), LANES)
    normed = rows_ref[:, lanes].astype(jnp.float32) * scale * gain_ref[:, lanes]
    expert = lax.broadcasted_iota(jnp.int32, (LANES, total), 0)
    named = [
        jnp.where(routes_ref[k : k + 1, :] == expert, 1.0, 0.0)
        for k in range(routes_ref.shape[0])
    ]
    earlier = lax.broadcasted_iota(jnp.int32, (total, total), 0) < lax.broadcasted_iota(
        jnp.int32, (total, total), 1
    )
    before = mm(sum(named), jnp.where(earlier, 1.0, 0.0))
    slot = lax.broadcasted_iota(jnp.int32, (slots, total), 0)
    chosen = jnp.zeros((slots, total), jnp.float32)
    combine = jnp.zeros((slots, total), jnp.float32)
    for k, one in enumerate(named):
        place = jnp.sum(before * one, axis=0, keepdims=True).astype(jnp.int32)
        hit = routes_ref[k : k + 1, :] * capacity + place == slot
        chosen = jnp.where(hit, 1.0, chosen)
        combine = jnp.where(hit, weight_ref[k : k + 1, :], combine)
    outgoing_ref[...] = mm(chosen, normed).astype(jnp.bfloat16)
    combine_ref[...] = combine.astype(jnp.bfloat16)


def routed(at, rows, gain, routes, weight, slots, capacity):
    total = rows.shape[0]
    whole = lambda array: pl.BlockSpec(array.shape, lambda: (0, 0))
    return pl.pallas_call(
        functools.partial(route_kernel, capacity),
        out_shape=(
            jax.ShapeDtypeStruct((slots, LANES), jnp.bfloat16),
            jax.ShapeDtypeStruct((slots, total), jnp.bfloat16),
        ),
        in_specs=in_vmem(0, 1) + [whole(v) for v in (rows, gain, routes, weight)],
        cost_estimate=pl.CostEstimate(
            flops=4 * total * slots * LANES, bytes_accessed=2 * rows.size, transcendentals=total
        ),
        compiler_params=pltpu.CompilerParams(vmem_limit_bytes=63600000),
        name="route_rows",
    )(at, rows, gain, routes, weight)


def summed_pieces(pieces):
    return jnp.sum(pieces.astype(jnp.float32), axis=0).astype(jnp.bfloat16)


def spread(array, axis):
    return lax.all_to_all(array, axis, 0, 0, tiled=True)


def on_device(
    query_in,
    key_in,
    value_in,
    erase_pre,
    decay_pre,
    mix_gain,
    expert_in,
    expert_gain,
    routes,
    route_weight,
    gate_weight,
    up_weight,
    down_weight,
):
    experts_n, shares = lax.axis_size("ep"), lax.axis_size("tp")
    row_count, features = expert_in.shape
    capacity = 3 * routes.shape[1] * row_count // (2 * experts_n)
    slot_total = experts_n * capacity
    col_count = features // shares
    at = lax.axis_index("tp") * col_count
    outgoing, combine = routed(
        at.reshape(1).astype(jnp.int32),
        expert_in,
        expert_gain[None],
        routes.T,
        route_weight.T,
        slot_total,
        capacity,
    )
    arrived = spread(outgoing.reshape(experts_n, capacity, col_count), "ep").reshape(
        slot_total, col_count
    )
    oloc, qp, own_maps = local_half(query_in, key_in, value_in, erase_pre, decay_pre)
    arrived, own_maps = lax.optimization_barrier((arrived, own_maps))
    middle = slot_total // 2
    copies = [
        jnp.broadcast_to(part[None], (shares, *part.shape))
        for part in (arrived[:middle], arrived[middle:])
    ]
    copies, own_maps = lax.optimization_barrier((copies, own_maps))
    shared_a = spread(copies[0], "tp")
    weights = [gate_weight[0].T, up_weight[0].T, down_weight[0]]
    shared_a, copies, own_maps = lax.optimization_barrier((shared_a, copies, own_maps))
    past, through = jnp.zeros(own_maps.shape, jnp.float32), own_maps

    def scanned(steps, past, through):
        for step in steps:
            past, through = scan_step(side(step), swapped(through, step), through, past)
        return past, through

    shared_b = spread(copies[1], "tp")
    partial_a = expert_rows(shared_a, *weights)
    past, through = scanned((1, 2), past, through)
    shared_b, partial_a, past, through = lax.optimization_barrier(
        (shared_b, partial_a, past, through)
    )
    pieces_a = spread(partial_a, "tp")
    partial_b = expert_rows(shared_b, *weights)
    past, through = scanned((4, 8), past, through)
    pieces_a, partial_b, past, through = lax.optimization_barrier(
        (pieces_a, partial_b, past, through)
    )
    pieces_b = spread(partial_b, "tp")
    summed_a = summed_pieces(pieces_a)
    distance = experts_n // 2
    crossing = swapped(through, distance)
    pieces_b, summed_a, crossing = lax.optimization_barrier((pieces_b, summed_a, crossing))
    summed = jnp.concatenate([summed_a, summed_pieces(pieces_b)], axis=0)
    returned = spread(summed.reshape(experts_n, capacity, col_count), "ep").reshape(
        slot_total, col_count
    )
    mixer_out = finish_half(side(distance), crossing, past, oloc, qp, mix_gain[:, None])
    expert_out = mm_tn(combine, returned).astype(jnp.bfloat16)
    return (mixer_out, expert_out)


def solution(mesh):
    placed = (
        P("tp", "ep"),
        P("tp", "ep"),
        P("tp", "ep"),
        P("tp", "ep"),
        P("tp", "ep"),
        P("tp"),
        P("ep", None),
        P(),
        P("ep", None),
        P("ep", None),
        P("ep", None, "tp"),
        P("ep", None, "tp"),
        P("ep", "tp", None),
    )
    return jax.shard_map(
        on_device,
        mesh=mesh,
        in_specs=placed,
        out_specs=(P("tp", "ep"), P("ep", "tp")),
        check_vma=False,
    )
```

```python
import functools

import jax
import jax.numpy as jnp
from jax import lax
from jax.experimental import pallas as pl
from jax.experimental.pallas import tpu as pltpu
from jax.sharding import PartitionSpec as P

HEAD_DIM = 64
LANES = 128
SPAN = 128
UNROLL = 2
DECAY_SCALE = 0.6065306597126334


def mm(a, b):
    return jnp.dot(
        a.astype(jnp.bfloat16), b.astype(jnp.bfloat16), preferred_element_type=jnp.float32
    )


def mm_tn(a, b):
    return lax.dot_general(
        a.astype(jnp.bfloat16),
        b.astype(jnp.bfloat16),
        (((0,), (0,)), ((), ())),
        preferred_element_type=jnp.float32,
    )


def mm_nt(a, b):
    return lax.dot_general(
        a.astype(jnp.bfloat16),
        b.astype(jnp.bfloat16),
        (((1,), (1,)), ((), ())),
        preferred_element_type=jnp.float32,
    )


def local_kernel(
    q_ref, k_ref, v_ref, e_ref, d_ref, oloc_ref, qp_ref, maps_ref,
    uk_ref, er_ref, lk_ref, qh_f_ref, qh_b_ref, z_ref, b_ref, dec_ref,
):
    count = q_ref.shape[1] // SPAN
    kf = k_ref[...].astype(jnp.float32)
    uk = kf * lax.rsqrt(jnp.sum(kf * kf, axis=0, keepdims=True) + 1e-05)
    uk_ref[...] = uk
    er_ref[...] = uk * (1.0 / (1.0 + jnp.exp(-e_ref[...].astype(jnp.float32))))
    lk_ref[...] = -DECAY_SCALE / (1.0 + jnp.exp(-d_ref[...].astype(jnp.float32)))

    row = lax.broadcasted_iota(jnp.int32, (SPAN, SPAN), 0)
    col = lax.broadcasted_iota(jnp.int32, (SPAN, SPAN), 1)
    differ = row ^ col
    eye_span = jnp.where(differ == 0, 1.0, 0.0)
    running = jnp.where(row <= col, 1.0, 0.0).astype(jnp.bfloat16)
    eye = jnp.where(
        lax.broadcasted_iota(jnp.int32, (HEAD_DIM, HEAD_DIM), 0)
        == lax.broadcasted_iota(jnp.int32, (HEAD_DIM, HEAD_DIM), 1),
        1.0,
        0.0,
    )
    strict = (row < col, row > col)
    inclusive = (row <= col, row >= col)

    def body(step, carry):
        units = []
        for part in range(UNROLL):
            chunk = step * UNROLL + part
            lanes = pl.ds(pl.multiple_of(chunk * SPAN, SPAN), SPAN)
            q = q_ref[:, lanes].astype(jnp.float32)
            k = k_ref[:, lanes].astype(jnp.float32)
            v = v_ref[:, lanes]
            u, er, lk = uk_ref[:, lanes], er_ref[:, lanes], lk_ref[:, lanes]
            high = lk.astype(jnp.bfloat16)
            rest = lk - high.astype(jnp.float32)
            low = rest.astype(jnp.bfloat16)
            sums = mm(jnp.concatenate([high, low], axis=0), running)
            cum = sums[:HEAD_DIM] + sums[HEAD_DIM:]
            prior = cum - lk
            last = cum[:, SPAN - 1 :]
            to_prior, fade = jnp.exp(prior), jnp.exp(last - cum)
            up_f, up_b = jnp.exp(-cum), jnp.exp(prior - last)
            dec_ref[chunk] = jnp.sum(eye * jnp.exp(last), axis=0, keepdims=True)
            both = (
                (u * to_prior, q * jnp.exp(cum), k * up_f, er * up_f, k * fade, er * fade),
                (u * fade, q * jnp.exp(last - prior), k * up_b, er * up_b, k * to_prior, er * to_prior),
            )
            for way in (0, 1):
                units.append((chunk, lanes, way, v, both[way]))
        state = []
        for chunk, lanes, way, v, (ud, qd, ku, eu, kend, eend) in units:
            gram = mm_tn(
                jnp.concatenate([ku, eu], axis=1), jnp.concatenate([ud, qd], axis=1)
            )
            k_mix = jnp.where(strict[way], gram[:SPAN, :SPAN], 0.0).astype(jnp.bfloat16)
            k_read = jnp.where(inclusive[way], gram[:SPAN, SPAN:], 0.0).astype(jnp.bfloat16)
            e_mix = jnp.where(strict[way], gram[SPAN:, :SPAN], 0.0)
            e_read = jnp.where(inclusive[way], gram[SPAN:, SPAN:], 0.0).astype(jnp.bfloat16)
            inv = (eye_span - jnp.where(differ == 1, e_mix, 0.0)).astype(jnp.bfloat16)
            mixed = mm(v, jnp.concatenate([k_mix, k_read], axis=1))
            state.append([e_mix, inv, mixed, e_read])
        width = 2
        while width < SPAN:
            inside = (differ >= width) & (differ < 2 * width)
            halves = [mm(inv, jnp.where(inside, e_mix, 0.0)) for e_mix, inv, _, _ in state]
            for unit, half in zip(state, halves):
                unit[1] = (unit[1].astype(jnp.float32) - mm(half, unit[1])).astype(jnp.bfloat16)
            width *= 2
        for (chunk, lanes, way, v, (ud, qd, ku, eu, kend, eend)), (_, inv, mixed, e_read) in zip(
            units, state
        ):
            solved = mm(jnp.concatenate([ud, mixed[:, :SPAN]], axis=0), inv).astype(jnp.bfloat16)
            read = mm(solved, e_read)
            ends = mm_nt(solved, eend)
            qh = (qh_f_ref, qh_b_ref)[way]
            qh[:, lanes] = (qd - read[:HEAD_DIM]).astype(jnp.bfloat16)
            out = mixed[:, SPAN:] - read[HEAD_DIM:]
            if way == 0:
                oloc_ref[:, lanes] = out
            else:
                oloc_ref[:, lanes] += out
            z_ref[way, chunk] = ends[:HEAD_DIM].astype(jnp.bfloat16)
            b_ref[way, chunk] = mm_nt(v, kend) - ends[HEAD_DIM:]
        return carry

    lax.fori_loop(0, count // UNROLL, body, 0)

    start = jnp.concatenate([jnp.zeros_like(eye), eye], axis=0)
    carried = [start, start]
    for step in range(count):
        for way, qh in ((0, qh_f_ref), (1, qh_b_ref)):
            chunk = step if way == 0 else count - 1 - step
            lanes = slice(chunk * SPAN, (chunk + 1) * SPAN)
            now = carried[way]
            narrow = now.astype(jnp.bfloat16)
            read = mm(narrow, qh[:, lanes])
            oloc_ref[:, lanes] += read[:HEAD_DIM]
            qp_ref[way * HEAD_DIM : (way + 1) * HEAD_DIM, lanes] = read[HEAD_DIM:].astype(jnp.bfloat16)
            moved = now * dec_ref[chunk] - mm(narrow, z_ref[way, chunk])
            carried[way] = jnp.concatenate(
                [moved[:HEAD_DIM] + b_ref[way, chunk], moved[HEAD_DIM:]], axis=0
            )
    for way in (0, 1):
        maps_ref[way] = jnp.concatenate(
            [carried[way][:HEAD_DIM], carried[way][HEAD_DIM:] - eye], axis=1
        ).astype(jnp.bfloat16)


def local_half(query, key, value, erase, decay):
    tokens = query.shape[1]
    count = tokens // SPAN
    full = lambda kind: jax.ShapeDtypeStruct((HEAD_DIM, tokens), kind)
    whole = lambda kind: pltpu.VMEM((HEAD_DIM, tokens), kind)
    return pl.pallas_call(
        local_kernel,
        out_shape=(
            full(jnp.float32),
            jax.ShapeDtypeStruct((2 * HEAD_DIM, tokens), jnp.bfloat16),
            jax.ShapeDtypeStruct((2, HEAD_DIM, 2 * HEAD_DIM), jnp.bfloat16),
        ),
        scratch_shapes=[
            whole(jnp.float32),
            whole(jnp.float32),
            whole(jnp.float32),
            whole(jnp.bfloat16),
            whole(jnp.bfloat16),
            pltpu.VMEM((2, count, HEAD_DIM, HEAD_DIM), jnp.bfloat16),
            pltpu.VMEM((2, count, HEAD_DIM, HEAD_DIM), jnp.float32),
            pltpu.VMEM((count, 1, HEAD_DIM), jnp.float32),
        ],
        cost_estimate=pl.CostEstimate(
            flops=16 * 22 * 2 * 128**3, bytes_accessed=tokens * 64 * 18, transcendentals=tokens * 64 * 9
        ),
        compiler_params=pltpu.CompilerParams(vmem_limit_bytes=66000000),
        name="mixer_local",
    )(query, key, value, erase, decay)


def stacked(wide):
    left = lax.broadcasted_iota(jnp.int32, (2 * HEAD_DIM, 2 * HEAD_DIM), 1) < HEAD_DIM
    full = wide.astype(jnp.float32)
    return jnp.where(left, jnp.concatenate([pltpu.roll(full, HEAD_DIM, 1), full], axis=0), 0.0)


def widened(tall):
    return tall[HEAD_DIM:] + pltpu.roll(tall[:HEAD_DIM], HEAD_DIM, 1)


def composed(first, later):
    return first + mm(first, later) + later


def step_kernel(upper_ref, arrived_ref, through_ref, past_ref, next_past_ref, next_through_ref):
    upper = upper_ref[0] != 0
    other = [stacked(arrived_ref[way]) for way in (0, 1)]
    mine = [stacked(through_ref[way]) for way in (0, 1)]
    near = jnp.where(upper, past_ref[0], past_ref[1])
    met = widened(composed(jnp.where(upper, other[0], other[1]), stacked(near)))
    next_past_ref[0] = jnp.where(upper, met, past_ref[0])
    next_past_ref[1] = jnp.where(upper, past_ref[1], met)
    for way in (0, 1):
        other_first = upper if way == 0 else jnp.logical_not(upper)
        first = jnp.where(other_first, other[way], mine[way])
        later = jnp.where(other_first, mine[way], other[way])
        next_through_ref[way] = widened(composed(first, later)).astype(jnp.bfloat16)


def in_vmem(count, scalars):
    return [pl.BlockSpec(memory_space=pltpu.SMEM)] * scalars + [
        pl.BlockSpec(memory_space=pltpu.VMEM)
    ] * count


def scan_step(upper, arrived, through, past, grant):
    return pl.pallas_call(
        step_kernel,
        out_shape=(
            jax.ShapeDtypeStruct(past.shape, jnp.float32),
            jax.ShapeDtypeStruct(past.shape, jnp.bfloat16),
        ),
        in_specs=in_vmem(3, 1),
        out_specs=tuple(in_vmem(2, 0)),
        cost_estimate=pl.CostEstimate(
            flops=6 * 128**3, bytes_accessed=6 * 2 * past.size, transcendentals=0
        ),
        compiler_params=pltpu.CompilerParams(vmem_limit_bytes=grant),
        name="scan_step",
    )(upper, arrived, through, past)


def finish_kernel(upper_ref, arrived_ref, past_ref, oloc_ref, qp_ref, gain_ref, out_ref):
    upper = upper_ref[0] != 0
    other = jnp.where(upper, arrived_ref[0].astype(jnp.float32), arrived_ref[1].astype(jnp.float32))
    near = jnp.where(upper, past_ref[0], past_ref[1])
    met = composed(stacked(other), stacked(near))[HEAD_DIM:]
    kept = stacked(jnp.where(upper, past_ref[1], past_ref[0]))[HEAD_DIM:]
    ahead, behind = jnp.where(upper, met, kept), jnp.where(upper, kept, met)
    states = ahead + pltpu.roll(behind, HEAD_DIM, 1)
    summed = oloc_ref[...] + mm(states, qp_ref[...])
    center = jnp.mean(summed, axis=0, keepdims=True)
    away = summed - center
    spread = jnp.mean(away * away, axis=0, keepdims=True)
    out_ref[...] = (
        away * lax.rsqrt(spread + HEAD_DIM * 1e-05) * gain_ref[...]
    ).astype(jnp.bfloat16)


def finish_half(upper, arrived, past, oloc, qp, gain):
    return pl.pallas_call(
        finish_kernel,
        out_shape=jax.ShapeDtypeStruct(oloc.shape, jnp.bfloat16),
        in_specs=in_vmem(5, 1),
        out_specs=in_vmem(1, 0)[0],
        cost_estimate=pl.CostEstimate(
            flops=4 * 128**3 + 16 * 128**3, bytes_accessed=2**20, transcendentals=1024
        ),
        compiler_params=pltpu.CompilerParams(vmem_limit_bytes=8 * 2**20),
        name="mixer_finish",
    )(upper, arrived, past, oloc, qp, gain)


def swapped(through, distance):
    count = lax.axis_size("ep")
    return lax.ppermute(through, "ep", [(i, i ^ distance) for i in range(count)])


def side(distance):
    return (lax.axis_index("ep") & distance).reshape(1).astype(jnp.int32)


def expert_kernel(rows_ref, gate_ref, up_ref, down_ref, out_ref):
    parts = rows_ref.shape[0]
    rows = jnp.concatenate([rows_ref[j] for j in range(parts)], axis=1)
    gate = mm_nt(rows, gate_ref[...])
    up = mm_nt(rows, up_ref[...])
    hidden = (gate / (1.0 + jnp.exp(-gate)) * up).astype(jnp.bfloat16)
    result = mm(hidden, down_ref[...]).astype(jnp.bfloat16)
    for j in range(parts):
        out_ref[j] = result[:, j * LANES : (j + 1) * LANES]


def expert_rows(rows, gate, up, down):
    parts, total, lanes = rows.shape
    tile = 192 if total % 192 == 0 else total
    block = pl.BlockSpec((parts, tile, lanes), lambda i: (0, i, 0))
    fixed = lambda array: pl.BlockSpec(array.shape, lambda i: (0, 0))
    return pl.pallas_call(
        expert_kernel,
        grid=(total // tile,),
        in_specs=[block, fixed(gate), fixed(up), fixed(down)],
        out_specs=block,
        out_shape=jax.ShapeDtypeStruct(rows.shape, jnp.bfloat16),
        cost_estimate=pl.CostEstimate(
            flops=6 * total * gate.size,
            bytes_accessed=2 * (2 * rows.size + 3 * gate.size),
            transcendentals=total * gate.shape[0],
        ),
        compiler_params=pltpu.CompilerParams(vmem_limit_bytes=66000000),
        name="expert_rows",
    )(rows, gate, up, down)


def route_kernel(
    capacity, at_ref, rows_ref, gain_ref, routes_ref, weight_ref, outgoing_ref, combine_ref
):
    slots, total = combine_ref.shape
    full = rows_ref[...].astype(jnp.float32)
    scale = lax.rsqrt(jnp.mean(full * full, axis=1, keepdims=True) + 1e-06)
    lanes = pl.ds(pl.multiple_of(at_ref[0], LANES), LANES)
    normed = rows_ref[:, lanes].astype(jnp.float32) * scale * gain_ref[:, lanes]
    expert = lax.broadcasted_iota(jnp.int32, (LANES, total), 0)
    named = [
        jnp.where(routes_ref[k : k + 1, :] == expert, 1.0, 0.0)
        for k in range(routes_ref.shape[0])
    ]
    earlier = lax.broadcasted_iota(jnp.int32, (total, total), 0) < lax.broadcasted_iota(
        jnp.int32, (total, total), 1
    )
    before = mm(sum(named), jnp.where(earlier, 1.0, 0.0))
    slot = lax.broadcasted_iota(jnp.int32, (slots, total), 0)
    chosen = jnp.zeros((slots, total), jnp.float32)
    combine = jnp.zeros((slots, total), jnp.float32)
    for k, one in enumerate(named):
        place = jnp.sum(before * one, axis=0, keepdims=True).astype(jnp.int32)
        hit = routes_ref[k : k + 1, :] * capacity + place == slot
        chosen = jnp.where(hit, 1.0, chosen)
        combine = jnp.where(hit, weight_ref[k : k + 1, :], combine)
    outgoing_ref[...] = mm(chosen, normed).astype(jnp.bfloat16)
    combine_ref[...] = combine.astype(jnp.bfloat16)


def routed(at, rows, gain, routes, weight, slots, capacity):
    total = rows.shape[0]
    whole = lambda array: pl.BlockSpec(array.shape, lambda: (0, 0))
    return pl.pallas_call(
        functools.partial(route_kernel, capacity),
        out_shape=(
            jax.ShapeDtypeStruct((slots, LANES), jnp.bfloat16),
            jax.ShapeDtypeStruct((slots, total), jnp.bfloat16),
        ),
        in_specs=in_vmem(0, 1) + [whole(v) for v in (rows, gain, routes, weight)],
        cost_estimate=pl.CostEstimate(
            flops=4 * total * slots * LANES, bytes_accessed=2 * rows.size, transcendentals=total
        ),
        compiler_params=pltpu.CompilerParams(vmem_limit_bytes=63600000),
        name="route_rows",
    )(at, rows, gain, routes, weight)


def summed_pieces(pieces):
    return jnp.sum(pieces.astype(jnp.float32), axis=0).astype(jnp.bfloat16)


def spread(array, axis):
    return lax.all_to_all(array, axis, 0, 0, tiled=True)


def on_device(
    query_in,
    key_in,
    value_in,
    erase_pre,
    decay_pre,
    mix_gain,
    expert_in,
    expert_gain,
    routes,
    route_weight,
    gate_weight,
    up_weight,
    down_weight,
):
    experts_n, shares = lax.axis_size("ep"), lax.axis_size("tp")
    row_count, features = expert_in.shape
    capacity = 3 * routes.shape[1] * row_count // (2 * experts_n)
    slot_total = experts_n * capacity
    col_count = features // shares
    at = lax.axis_index("tp") * col_count
    outgoing, combine = routed(
        at.reshape(1).astype(jnp.int32),
        expert_in,
        expert_gain[None],
        routes.T,
        route_weight.T,
        slot_total,
        capacity,
    )
    arrived = spread(outgoing.reshape(experts_n, capacity, col_count), "ep").reshape(
        slot_total, col_count
    )
    oloc, qp, own_maps = local_half(query_in, key_in, value_in, erase_pre, decay_pre)
    arrived, own_maps = lax.optimization_barrier((arrived, own_maps))
    middle = slot_total // 2
    copies = [
        jnp.broadcast_to(part[None], (shares, *part.shape))
        for part in (arrived[:middle], arrived[middle:])
    ]
    copies[0], own_maps = lax.optimization_barrier((copies[0], own_maps))
    shared_a = spread(copies[0], "tp")
    past, through = jnp.zeros(own_maps.shape, jnp.float32), own_maps
    weights = [gate_weight[0].T, up_weight[0].T, down_weight[0]]

    def scanned(steps, past, through):
        for step in steps:
            grant = 66000000 if step < 4 else 4 * 2**20
            past, through = scan_step(side(step), swapped(through, step), through, past, grant)
        return past, through

    past, through = scanned((1,), past, through)
    copies[1], past, through = lax.optimization_barrier((copies[1], past, through))
    past, through = scanned((2,), past, through)
    shared_a, copies[1], past, through = lax.optimization_barrier(
        (shared_a, copies[1], past, through)
    )
    shared_b = spread(copies[1], "tp")
    partial_a = expert_rows(shared_a, *weights)
    past, through = scanned((4,), past, through)
    shared_b, partial_a, past, through = lax.optimization_barrier(
        (shared_b, partial_a, past, through)
    )
    pieces_a = spread(partial_a, "tp")
    partial_b = expert_rows(shared_b, *weights)
    past, through = scanned((8,), past, through)
    pieces_a, partial_b, past, through = lax.optimization_barrier(
        (pieces_a, partial_b, past, through)
    )
    pieces_b = spread(partial_b, "tp")
    summed_a = summed_pieces(pieces_a)
    distance = experts_n // 2
    crossing = swapped(through, distance)
    pieces_b, summed_a, crossing = lax.optimization_barrier((pieces_b, summed_a, crossing))
    summed = jnp.concatenate([summed_a, summed_pieces(pieces_b)], axis=0)
    returned = spread(summed.reshape(experts_n, capacity, col_count), "ep").reshape(
        slot_total, col_count
    )
    mixer_out = finish_half(side(distance), crossing, past, oloc, qp, mix_gain[:, None])
    expert_out = mm_tn(combine, returned).astype(jnp.bfloat16)
    return (mixer_out, expert_out)


def solution(mesh):
    placed = (
        P("tp", "ep"),
        P("tp", "ep"),
        P("tp", "ep"),
        P("tp", "ep"),
        P("tp", "ep"),
        P("tp"),
        P("ep", None),
        P(),
        P("ep", None),
        P("ep", None),
        P("ep", None, "tp"),
        P("ep", None, "tp"),
        P("ep", "tp", None),
    )
    return jax.shard_map(
        on_device,
        mesh=mesh,
        in_specs=placed,
        out_specs=(P("tp", "ep"), P("ep", "tp")),
        check_vma=False,
    )
```

```python
import functools

import jax
import jax.numpy as jnp
from jax import lax
from jax.experimental import pallas as pl
from jax.experimental.pallas import tpu as pltpu
from jax.sharding import PartitionSpec as P

HEAD_DIM = 64
LANES = 128
SPAN = 128
UNROLL = 2
DECAY_SCALE = 0.6065306597126334


def mm(a, b):
    return jnp.dot(
        a.astype(jnp.bfloat16), b.astype(jnp.bfloat16), preferred_element_type=jnp.float32
    )


def mm_tn(a, b):
    return lax.dot_general(
        a.astype(jnp.bfloat16),
        b.astype(jnp.bfloat16),
        (((0,), (0,)), ((), ())),
        preferred_element_type=jnp.float32,
    )


def mm_nt(a, b):
    return lax.dot_general(
        a.astype(jnp.bfloat16),
        b.astype(jnp.bfloat16),
        (((1,), (1,)), ((), ())),
        preferred_element_type=jnp.float32,
    )


def local_kernel(
    q_ref, k_ref, v_ref, e_ref, d_ref, oloc_ref, qp_ref, maps_ref,
    uk_ref, er_ref, lk_ref, qh_f_ref, qh_b_ref, z_ref, b_ref, dec_ref,
):
    count = q_ref.shape[1] // SPAN
    kf = k_ref[...].astype(jnp.float32)
    uk = kf * lax.rsqrt(jnp.sum(kf * kf, axis=0, keepdims=True) + 1e-05)
    uk_ref[...] = uk
    er_ref[...] = uk * (1.0 / (1.0 + jnp.exp(-e_ref[...].astype(jnp.float32))))
    lk_ref[...] = -DECAY_SCALE / (1.0 + jnp.exp(-d_ref[...].astype(jnp.float32)))

    row = lax.broadcasted_iota(jnp.int32, (SPAN, SPAN), 0)
    col = lax.broadcasted_iota(jnp.int32, (SPAN, SPAN), 1)
    differ = row ^ col
    eye_span = jnp.where(differ == 0, 1.0, 0.0)
    running = jnp.where(row <= col, 1.0, 0.0).astype(jnp.bfloat16)
    eye = jnp.where(
        lax.broadcasted_iota(jnp.int32, (HEAD_DIM, HEAD_DIM), 0)
        == lax.broadcasted_iota(jnp.int32, (HEAD_DIM, HEAD_DIM), 1),
        1.0,
        0.0,
    )
    strict = (row < col, row > col)
    inclusive = (row <= col, row >= col)

    def body(step, carry):
        units = []
        for part in range(UNROLL):
            chunk = step * UNROLL + part
            lanes = pl.ds(pl.multiple_of(chunk * SPAN, SPAN), SPAN)
            q = q_ref[:, lanes].astype(jnp.float32)
            k = k_ref[:, lanes].astype(jnp.float32)
            v = v_ref[:, lanes]
            u, er, lk = uk_ref[:, lanes], er_ref[:, lanes], lk_ref[:, lanes]
            high = lk.astype(jnp.bfloat16)
            rest = lk - high.astype(jnp.float32)
            low = rest.astype(jnp.bfloat16)
            sums = mm(jnp.concatenate([high, low], axis=0), running)
            cum = sums[:HEAD_DIM] + sums[HEAD_DIM:]
            prior = cum - lk
            last = cum[:, SPAN - 1 :]
            to_prior, fade = jnp.exp(prior), jnp.exp(last - cum)
            up_f, up_b = jnp.exp(-cum), jnp.exp(prior - last)
            dec_ref[chunk] = jnp.sum(eye * jnp.exp(last), axis=0, keepdims=True)
            both = (
                (u * to_prior, q * jnp.exp(cum), k * up_f, er * up_f, k * fade, er * fade),
                (u * fade, q * jnp.exp(last - prior), k * up_b, er * up_b, k * to_prior, er * to_prior),
            )
            for way in (0, 1):
                units.append((chunk, lanes, way, v, both[way]))
        state = []
        for chunk, lanes, way, v, (ud, qd, ku, eu, kend, eend) in units:
            gram = mm_tn(
                jnp.concatenate([ku, eu], axis=1), jnp.concatenate([ud, qd], axis=1)
            )
            k_mix = jnp.where(strict[way], gram[:SPAN, :SPAN], 0.0).astype(jnp.bfloat16)
            k_read = jnp.where(inclusive[way], gram[:SPAN, SPAN:], 0.0).astype(jnp.bfloat16)
            e_mix = jnp.where(strict[way], gram[SPAN:, :SPAN], 0.0)
            e_read = jnp.where(inclusive[way], gram[SPAN:, SPAN:], 0.0).astype(jnp.bfloat16)
            inv = (eye_span - jnp.where(differ == 1, e_mix, 0.0)).astype(jnp.bfloat16)
            mixed = mm(v, jnp.concatenate([k_mix, k_read], axis=1))
            state.append([e_mix, inv, mixed, e_read])
        width = 2
        while width < SPAN:
            inside = (differ >= width) & (differ < 2 * width)
            halves = [mm(inv, jnp.where(inside, e_mix, 0.0)) for e_mix, inv, _, _ in state]
            for unit, half in zip(state, halves):
                unit[1] = (unit[1].astype(jnp.float32) - mm(half, unit[1])).astype(jnp.bfloat16)
            width *= 2
        for (chunk, lanes, way, v, (ud, qd, ku, eu, kend, eend)), (_, inv, mixed, e_read) in zip(
            units, state
        ):
            solved = mm(jnp.concatenate([ud, mixed[:, :SPAN]], axis=0), inv).astype(jnp.bfloat16)
            read = mm(solved, e_read)
            ends = mm_nt(solved, eend)
            qh = (qh_f_ref, qh_b_ref)[way]
            qh[:, lanes] = (qd - read[:HEAD_DIM]).astype(jnp.bfloat16)
            out = mixed[:, SPAN:] - read[HEAD_DIM:]
            if way == 0:
                oloc_ref[:, lanes] = out
            else:
                oloc_ref[:, lanes] += out
            z_ref[way, chunk] = ends[:HEAD_DIM].astype(jnp.bfloat16)
            b_ref[way, chunk] = mm_nt(v, kend) - ends[HEAD_DIM:]
        return carry

    lax.fori_loop(0, count // UNROLL, body, 0)

    start = jnp.concatenate([jnp.zeros_like(eye), eye], axis=0)
    carried = [start, start]
    for step in range(count):
        for way, qh in ((0, qh_f_ref), (1, qh_b_ref)):
            chunk = step if way == 0 else count - 1 - step
            lanes = slice(chunk * SPAN, (chunk + 1) * SPAN)
            now = carried[way]
            narrow = now.astype(jnp.bfloat16)
            read = mm(narrow, qh[:, lanes])
            oloc_ref[:, lanes] += read[:HEAD_DIM]
            qp_ref[way * HEAD_DIM : (way + 1) * HEAD_DIM, lanes] = read[HEAD_DIM:].astype(jnp.bfloat16)
            moved = now * dec_ref[chunk] - mm(narrow, z_ref[way, chunk])
            carried[way] = jnp.concatenate(
                [moved[:HEAD_DIM] + b_ref[way, chunk], moved[HEAD_DIM:]], axis=0
            )
    for way in (0, 1):
        maps_ref[way] = jnp.concatenate(
            [carried[way][:HEAD_DIM], carried[way][HEAD_DIM:] - eye], axis=1
        ).astype(jnp.bfloat16)


def local_half(query, key, value, erase, decay):
    tokens = query.shape[1]
    count = tokens // SPAN
    full = lambda kind: jax.ShapeDtypeStruct((HEAD_DIM, tokens), kind)
    whole = lambda kind: pltpu.VMEM((HEAD_DIM, tokens), kind)
    return pl.pallas_call(
        local_kernel,
        out_shape=(
            full(jnp.float32),
            jax.ShapeDtypeStruct((2 * HEAD_DIM, tokens), jnp.bfloat16),
            jax.ShapeDtypeStruct((2, HEAD_DIM, 2 * HEAD_DIM), jnp.bfloat16),
        ),
        scratch_shapes=[
            whole(jnp.float32),
            whole(jnp.float32),
            whole(jnp.float32),
            whole(jnp.bfloat16),
            whole(jnp.bfloat16),
            pltpu.VMEM((2, count, HEAD_DIM, HEAD_DIM), jnp.bfloat16),
            pltpu.VMEM((2, count, HEAD_DIM, HEAD_DIM), jnp.float32),
            pltpu.VMEM((count, 1, HEAD_DIM), jnp.float32),
        ],
        cost_estimate=pl.CostEstimate(
            flops=16 * 22 * 2 * 128**3, bytes_accessed=tokens * 64 * 18, transcendentals=tokens * 64 * 9
        ),
        compiler_params=pltpu.CompilerParams(vmem_limit_bytes=66000000),
        name="mixer_local",
    )(query, key, value, erase, decay)


def stacked(wide):
    left = lax.broadcasted_iota(jnp.int32, (2 * HEAD_DIM, 2 * HEAD_DIM), 1) < HEAD_DIM
    full = wide.astype(jnp.float32)
    return jnp.where(left, jnp.concatenate([pltpu.roll(full, HEAD_DIM, 1), full], axis=0), 0.0)


def widened(tall):
    return tall[HEAD_DIM:] + pltpu.roll(tall[:HEAD_DIM], HEAD_DIM, 1)


def composed(first, later):
    return first + mm(first, later) + later


def step_kernel(upper_ref, arrived_ref, through_ref, past_ref, next_past_ref, next_through_ref):
    upper = upper_ref[0] != 0
    other = [stacked(arrived_ref[way]) for way in (0, 1)]
    mine = [stacked(through_ref[way]) for way in (0, 1)]
    near = jnp.where(upper, past_ref[0], past_ref[1])
    met = widened(composed(jnp.where(upper, other[0], other[1]), stacked(near)))
    next_past_ref[0] = jnp.where(upper, met, past_ref[0])
    next_past_ref[1] = jnp.where(upper, past_ref[1], met)
    for way in (0, 1):
        other_first = upper if way == 0 else jnp.logical_not(upper)
        first = jnp.where(other_first, other[way], mine[way])
        later = jnp.where(other_first, mine[way], other[way])
        next_through_ref[way] = widened(composed(first, later)).astype(jnp.bfloat16)


def in_vmem(count, scalars):
    return [pl.BlockSpec(memory_space=pltpu.SMEM)] * scalars + [
        pl.BlockSpec(memory_space=pltpu.VMEM)
    ] * count


def scan_step(upper, arrived, through, past):
    return pl.pallas_call(
        step_kernel,
        out_shape=(
            jax.ShapeDtypeStruct(past.shape, jnp.float32),
            jax.ShapeDtypeStruct(past.shape, jnp.bfloat16),
        ),
        in_specs=in_vmem(3, 1),
        out_specs=tuple(in_vmem(2, 0)),
        cost_estimate=pl.CostEstimate(
            flops=6 * 128**3, bytes_accessed=6 * 2 * past.size, transcendentals=0
        ),
        compiler_params=pltpu.CompilerParams(vmem_limit_bytes=4 * 2**20),
        name="scan_step",
    )(upper, arrived, through, past)


def finish_kernel(upper_ref, arrived_ref, past_ref, oloc_ref, qp_ref, gain_ref, out_ref):
    upper = upper_ref[0] != 0
    other = jnp.where(upper, arrived_ref[0].astype(jnp.float32), arrived_ref[1].astype(jnp.float32))
    near = jnp.where(upper, past_ref[0], past_ref[1])
    met = composed(stacked(other), stacked(near))[HEAD_DIM:]
    kept = stacked(jnp.where(upper, past_ref[1], past_ref[0]))[HEAD_DIM:]
    ahead, behind = jnp.where(upper, met, kept), jnp.where(upper, kept, met)
    states = ahead + pltpu.roll(behind, HEAD_DIM, 1)
    summed = oloc_ref[...] + mm(states, qp_ref[...])
    center = jnp.mean(summed, axis=0, keepdims=True)
    away = summed - center
    spread = jnp.mean(away * away, axis=0, keepdims=True)
    out_ref[...] = (
        away * lax.rsqrt(spread + HEAD_DIM * 1e-05) * gain_ref[...]
    ).astype(jnp.bfloat16)


def finish_half(upper, arrived, past, oloc, qp, gain):
    return pl.pallas_call(
        finish_kernel,
        out_shape=jax.ShapeDtypeStruct(oloc.shape, jnp.bfloat16),
        in_specs=in_vmem(5, 1),
        out_specs=in_vmem(1, 0)[0],
        cost_estimate=pl.CostEstimate(
            flops=4 * 128**3 + 16 * 128**3, bytes_accessed=2**20, transcendentals=1024
        ),
        compiler_params=pltpu.CompilerParams(vmem_limit_bytes=8 * 2**20),
        name="mixer_finish",
    )(upper, arrived, past, oloc, qp, gain)


def swapped(through, distance):
    count = lax.axis_size("ep")
    return lax.ppermute(through, "ep", [(i, i ^ distance) for i in range(count)])


def side(distance):
    return (lax.axis_index("ep") & distance).reshape(1).astype(jnp.int32)


def expert_kernel(rows_ref, gate_ref, up_ref, down_ref, out_ref):
    parts = rows_ref.shape[0]
    rows = jnp.concatenate([rows_ref[j] for j in range(parts)], axis=1)
    gate = mm_nt(rows, gate_ref[...])
    up = mm_nt(rows, up_ref[...])
    hidden = (gate / (1.0 + jnp.exp(-gate)) * up).astype(jnp.bfloat16)
    result = mm(hidden, down_ref[...]).astype(jnp.bfloat16)
    for j in range(parts):
        out_ref[j] = result[:, j * LANES : (j + 1) * LANES]


def expert_rows(rows, gate, up, down):
    parts, total, lanes = rows.shape
    tile = 256 if total % 256 == 0 else total
    block = pl.BlockSpec((parts, tile, lanes), lambda i: (0, i, 0))
    fixed = lambda array: pl.BlockSpec(array.shape, lambda i: (0, 0))
    return pl.pallas_call(
        expert_kernel,
        grid=(total // tile,),
        in_specs=[block, fixed(gate), fixed(up), fixed(down)],
        out_specs=block,
        out_shape=jax.ShapeDtypeStruct(rows.shape, jnp.bfloat16),
        cost_estimate=pl.CostEstimate(
            flops=6 * total * gate.size,
            bytes_accessed=2 * (2 * rows.size + 3 * gate.size),
            transcendentals=total * gate.shape[0],
        ),
        compiler_params=pltpu.CompilerParams(vmem_limit_bytes=66000000),
        name="expert_rows",
    )(rows, gate, up, down)


def route_kernel(
    capacity, at_ref, rows_ref, gain_ref, routes_ref, weight_ref, outgoing_ref, combine_ref
):
    slots, total = combine_ref.shape
    full = rows_ref[...].astype(jnp.float32)
    scale = lax.rsqrt(jnp.mean(full * full, axis=1, keepdims=True) + 1e-06)
    lanes = pl.ds(pl.multiple_of(at_ref[0], LANES), LANES)
    normed = rows_ref[:, lanes].astype(jnp.float32) * scale * gain_ref[:, lanes]
    expert = lax.broadcasted_iota(jnp.int32, (LANES, total), 0)
    named = [
        jnp.where(routes_ref[k : k + 1, :] == expert, 1.0, 0.0)
        for k in range(routes_ref.shape[0])
    ]
    earlier = lax.broadcasted_iota(jnp.int32, (total, total), 0) < lax.broadcasted_iota(
        jnp.int32, (total, total), 1
    )
    before = mm(sum(named), jnp.where(earlier, 1.0, 0.0))
    slot = lax.broadcasted_iota(jnp.int32, (slots, total), 0)
    chosen = jnp.zeros((slots, total), jnp.float32)
    combine = jnp.zeros((slots, total), jnp.float32)
    for k, one in enumerate(named):
        place = jnp.sum(before * one, axis=0, keepdims=True).astype(jnp.int32)
        hit = routes_ref[k : k + 1, :] * capacity + place == slot
        chosen = jnp.where(hit, 1.0, chosen)
        combine = jnp.where(hit, weight_ref[k : k + 1, :], combine)
    outgoing_ref[...] = mm(chosen, normed).astype(jnp.bfloat16)
    combine_ref[...] = combine.astype(jnp.bfloat16)


def routed(at, rows, gain, routes, weight, slots, capacity):
    total = rows.shape[0]
    whole = lambda array: pl.BlockSpec(array.shape, lambda: (0, 0))
    return pl.pallas_call(
        functools.partial(route_kernel, capacity),
        out_shape=(
            jax.ShapeDtypeStruct((slots, LANES), jnp.bfloat16),
            jax.ShapeDtypeStruct((slots, total), jnp.bfloat16),
        ),
        in_specs=in_vmem(0, 1) + [whole(v) for v in (rows, gain, routes, weight)],
        cost_estimate=pl.CostEstimate(
            flops=4 * total * slots * LANES, bytes_accessed=2 * rows.size, transcendentals=total
        ),
        compiler_params=pltpu.CompilerParams(vmem_limit_bytes=63600000),
        name="route_rows",
    )(at, rows, gain, routes, weight)


def sum_kernel(pieces_ref, out_ref):
    parts, total, _ = pieces_ref.shape
    tile = 64 if total % 64 == 0 else total

    def body(step, carry):
        at = pl.ds(pl.multiple_of(step * tile, tile), tile)
        whole = pieces_ref[0, at, :].astype(jnp.float32)
        for j in range(1, parts):
            whole += pieces_ref[j, at, :].astype(jnp.float32)
        out_ref[at, :] = whole.astype(jnp.bfloat16)
        return carry

    lax.fori_loop(0, total // tile, body, 0)


def summed_pieces(pieces):
    return pl.pallas_call(
        sum_kernel,
        out_shape=jax.ShapeDtypeStruct(pieces.shape[1:], jnp.bfloat16),
        in_specs=in_vmem(1, 0),
        cost_estimate=pl.CostEstimate(
            flops=pieces.size, bytes_accessed=2 * pieces.size, transcendentals=0
        ),
        compiler_params=pltpu.CompilerParams(vmem_limit_bytes=4 * 2**20),
        name="sum_pieces",
    )(pieces)


def spread(array, axis):
    return lax.all_to_all(array, axis, 0, 0, tiled=True)


def on_device(
    query_in,
    key_in,
    value_in,
    erase_pre,
    decay_pre,
    mix_gain,
    expert_in,
    expert_gain,
    routes,
    route_weight,
    gate_weight,
    up_weight,
    down_weight,
):
    experts_n, shares = lax.axis_size("ep"), lax.axis_size("tp")
    row_count, features = expert_in.shape
    capacity = 3 * routes.shape[1] * row_count // (2 * experts_n)
    slot_total = experts_n * capacity
    col_count = features // shares
    at = lax.axis_index("tp") * col_count
    outgoing, combine = routed(
        at.reshape(1).astype(jnp.int32),
        expert_in,
        expert_gain[None],
        routes.T,
        route_weight.T,
        slot_total,
        capacity,
    )
    arrived = spread(outgoing.reshape(experts_n, capacity, col_count), "ep").reshape(
        slot_total, col_count
    )
    oloc, qp, own_maps = local_half(query_in, key_in, value_in, erase_pre, decay_pre)
    arrived, own_maps = lax.optimization_barrier((arrived, own_maps))
    copies = jnp.broadcast_to(arrived[None], (shares, *arrived.shape))
    copies, own_maps = lax.optimization_barrier((copies, own_maps))
    shared = spread(copies, "tp")
    past, through = jnp.zeros(own_maps.shape, jnp.float32), own_maps
    weights = [gate_weight[0].T, up_weight[0].T, down_weight[0]]

    def scanned(steps, past, through):
        for step in steps:
            past, through = scan_step(side(step), swapped(through, step), through, past)
        return past, through

    past, through = scanned((1, 2, 4), past, through)
    shared, past, through = lax.optimization_barrier((shared, past, through))
    partial = expert_rows(shared, *weights)
    partial, past, through = lax.optimization_barrier((partial, past, through))
    pieces = spread(partial, "tp")
    past, through = scanned((8,), past, through)
    distance = experts_n // 2
    crossing = swapped(through, distance)
    pieces, crossing = lax.optimization_barrier((pieces, crossing))
    summed = summed_pieces(pieces)
    returned = spread(summed.reshape(experts_n, capacity, col_count), "ep").reshape(
        slot_total, col_count
    )
    mixer_out = finish_half(side(distance), crossing, past, oloc, qp, mix_gain[:, None])
    expert_out = mm_tn(combine, returned).astype(jnp.bfloat16)
    return (mixer_out, expert_out)


def solution(mesh):
    placed = (
        P("tp", "ep"),
        P("tp", "ep"),
        P("tp", "ep"),
        P("tp", "ep"),
        P("tp", "ep"),
        P("tp"),
        P("ep", None),
        P(),
        P("ep", None),
        P("ep", None),
        P("ep", None, "tp"),
        P("ep", None, "tp"),
        P("ep", "tp", None),
    )
    return jax.shard_map(
        on_device,
        mesh=mesh,
        in_specs=placed,
        out_specs=(P("tp", "ep"), P("ep", "tp")),
        check_vma=False,
    )
```
